32 devices in a mesh: ep: 16 (over z, y, x), tp: 2 (over core).
Axes of the slice: x: 2, y: 2, z: 4, core: 2. Of those that a mesh axis runs over, the one named last changes fastest.
Arguments:
- inputs: bfloat16 [8192, 2048], P(('ep', 'tp')), may hold values from -6 to 6
- pre_gain: float32 [2048], replicated, may hold values from 0.5 to 8
- expert_ids: int32 [8192, 2], P(('ep', 'tp')), may hold values from 0 to 15, all different within a row; in each aligned block of 256 rows (0 to 255, 256 to 511, ...) at most 48 rows name the same one
- route_weights: float32 [8192, 2], P(('ep', 'tp')), may hold values from 0.05 to 1
- gate_proj: bfloat16 [16, 2048, 2048], P('ep', None, 'tp'), may hold values from -0.125 to 0.125
- up_proj: bfloat16 [16, 2048, 2048], P('ep', None, 'tp'), may hold values from -0.125 to 0.125
- down_proj: bfloat16 [16, 2048, 2048], P('ep', 'tp'), may hold values from -0.125 to 0.125
- post_gain: float32 [2048], replicated, may hold values from 0.1 to 1.9
Outputs:
- layer_out: bfloat16 [8192, 2048], P(('ep', 'tp'))
The draws below stay inside these ranges and needn't reach their ends.
Inputs may be any that keep to these rules, and one draw needn't show every extreme that they name: `expert_ids`: each token names 2 different experts. Among the 256 tokens of one device (aligned blocks of rows) no expert is named by more than 48 tokens, and in every draw some expert is named by exactly 48 tokens of some device.
All inputs are finite; a program needn't handle non-finite values.
Results may differ from the reference program's by a relative error of at most 0.0095.
Values may be sent and summed in bfloat16 or wider, within the bound.
A program may use at most 128 MiB of HBM per device.

```python
import math
import jax
import jax.numpy as jnp
import numpy as np
from jax import lax

D = 2048
FE = 2048
TOP_K = 2
TOK_DEV = 256
EXPERTS = 16
CAP = 48
TOKENS = 8192
N_EP = 16
N_TP = 2


def draw_pre_gain(key, part):
    return 1.0 + 0.18 * jnp.clip(jax.random.normal(key, (D,), jnp.float32), -2.5, 2.5)


def level_of(rng, dims, split, low, high):
    loudness = 1.0
    for dim, shards_of in split:
        steps = jax.random.uniform(jax.random.fold_in(jax.random.fold_in(rng, 6), dim), (shards_of,), jnp.float32, low / len(split), high / len(split))
        loudness = loudness * jnp.repeat(jnp.exp(steps), dims[dim] // shards_of).reshape((-1,) + (1,) * (len(dims) - 1 - dim))
    return loudness


def shared_out(stream_key, own, number, rows, count, top, reach, skew):
    sequence = jax.random.permutation(stream_key, count)
    packed, ordinary = shares(count, rows * top, reach, skew, True), shares(count, rows * top, reach, skew, False)
    places = jnp.arange(count)

    def named(tallies, turn):
        used = int((tallies > 0).sum())
        fixed = max(1, used // 4)
        moved = fixed + (places - fixed + turn * (used - fixed)) % max(1, count - fixed)
        return jnp.zeros((count,), jnp.int32).at[sequence[jnp.where(places < fixed, places, moved)]].set(jnp.asarray(tallies, jnp.int32))

    tallies = jnp.where(number % 4 == 0, named(packed, number // 4), named(ordinary, number - number // 4 - 1))
    mixed = jax.random.permutation(jax.random.fold_in(own, 3), count)
    giver, taker = mixed[0:count // 2 * 2:2], mixed[1:count // 2 * 2:2]
    margin = jnp.minimum(tallies[giver] - 1, reach - tallies[taker]) // 2
    margin = jnp.where((giver == sequence[0]) | (taker == sequence[0]) | (tallies[taker] == 0), 0, jnp.maximum(margin, 0))
    moved = jax.random.randint(jax.random.fold_in(own, 4), (count // 2,), 0, 1 << 20) % (margin + 1)
    tallies = tallies.at[giver].add(-moved).at[taker].add(moved)
    items = jnp.searchsorted(jnp.cumsum(tallies), jnp.arange(rows * top), side="right").astype(jnp.int32)
    listing = items.reshape(top, rows).T
    listing = listing[jax.random.permutation(jax.random.fold_in(own, 1), rows)]
    turn = jax.random.randint(jax.random.fold_in(own, 2), (rows, 1), 0, top)
    return jnp.take_along_axis(listing, (jnp.arange(top)[None, :] + turn) % top, axis=1)


def shares(amount, total, reach, lean, full):
    portions = [(1 << 20) // math.isqrt(standing ** lean) + 1 for standing in range(1, amount + 1)]
    largest = reach if full else min(reach, max(-(-total // amount), total * portions[0] // sum(portions)))
    least = 1 if total - largest >= amount - 1 else 0
    holding, surplus = [largest] + [least] * (amount - 1), total - largest - least * (amount - 1)
    while surplus > 0:
        movable = [i for i in range(1, amount) if holding[i] < largest] or [i for i in range(1, amount) if holding[i] < reach]
        whole, left = sum([portions[i] for i in movable]), surplus
        for i in movable:
            extra = min(reach - holding[i], max(1, left * portions[i] // whole), surplus)
            holding[i] = holding[i] + extra
            surplus = surplus - extra
    return np.array(holding)


def gaussian(key, shape, scale, most, shards=(), held_as=jnp.bfloat16):
    drawn = jax.random.normal(key, shape, jnp.float32) * scale
    if len(shards) > 0:
        drawn = level_of(key, shape, shards, -0.22, 0.18) * drawn
    return jnp.clip(drawn, min=-most, max=most).astype(held_as)


def setup_inputs(seed: int = 0) -> dict:
    keys = jax.random.split(jax.random.key(seed), 9)
    inputs = gaussian(keys[0], (TOKENS, D), 1.0, 6.0, ((0, 32),))
    pre_gain = draw_pre_gain(jax.random.fold_in(keys[8], 71), 0)
    expert_ids_keys = jax.random.split(jax.random.fold_in(keys[2], 1), TOKENS // TOK_DEV)
    expert_ids_turns = jax.random.permutation(jax.random.fold_in(keys[2], 3), TOKENS // TOK_DEV)
    expert_ids = jax.vmap(lambda own, number: shared_out(jax.random.fold_in(keys[2], 2), own, number, TOK_DEV, EXPERTS, TOP_K, CAP, 2))(expert_ids_keys, expert_ids_turns).reshape((TOKENS, TOP_K))
    route_weights = jnp.clip(jnp.exp(math.log(1.0) - 2.9957323 * jax.random.uniform(keys[3], (TOKENS, TOP_K), jnp.float32) ** level_of(keys[3], (TOKENS, TOP_K), ((0, 32),), -0.2, 0.2)), 0.05, 1.0)
    gate_proj = gaussian(keys[4], (EXPERTS, D, FE), D ** -0.5, 0.125, ((0, 16), (2, 2)))
    up_proj = gaussian(keys[5], (EXPERTS, D, FE), D ** -0.5, 0.125, ((0, 16), (2, 2)))
    down_proj = gaussian(keys[6], (EXPERTS, FE, D), FE ** -0.5, 0.125, ((0, 16), (1, 2)))
    post_gain = jnp.clip(1.0 + 0.18 * jax.random.normal(keys[7], (D,), jnp.float32), 0.1, 1.9)
    return {"inputs": inputs, "pre_gain": pre_gain, "expert_ids": expert_ids, "route_weights": route_weights, "gate_proj": gate_proj, "up_proj": up_proj, "down_proj": down_proj, "post_gain": post_gain}


EPSILON = 1e-06
LIMIT = 7.0
ALPHA = 1.702

def norm_rows(values, gain):
    floats = values.astype(jnp.float32)
    return floats * lax.rsqrt(lax.optimization_barrier(jnp.mean(floats * floats, axis=-1, keepdims=True)) + EPSILON) * gain

def activate(gate, up):
    gate = jnp.minimum(gate, LIMIT)
    up = jnp.clip(up, -LIMIT, LIMIT)
    return ((up + 1.0) * gate * jax.nn.sigmoid(ALPHA * gate)).astype(jnp.bfloat16)

def reference(inputs, pre_gain, expert_ids, route_weights, gate_proj, up_proj, down_proj, post_gain):
    devices_all = N_EP * N_TP
    normed = norm_rows(inputs, pre_gain).astype(jnp.bfloat16)
    blocks = expert_ids.reshape(devices_all, TOK_DEV * TOP_K)
    one_hot = (blocks[:, :, None] == jnp.arange(EXPERTS, dtype=jnp.int32)[None, None, :]).astype(jnp.int32)
    earlier = jnp.cumsum(one_hot, axis=1) - one_hot
    slot = lax.optimization_barrier(jnp.sum(earlier * one_hot, axis=-1))
    source = jnp.arange(devices_all, dtype=jnp.int32)[:, None]
    target = (blocks * (devices_all * CAP) + source * CAP + slot).reshape(-1).astype(jnp.int32)
    copies = jnp.repeat(normed, TOP_K, axis=0)
    buffer = jnp.zeros((EXPERTS * devices_all * CAP, D), jnp.bfloat16).at[target].set(copies)
    buffer = buffer.reshape(EXPERTS, devices_all * CAP, D)
    half = FE // N_TP

    def one_expert(operands):
        rows, w_gate, w_up, w_down = operands
        gate = jnp.dot(rows, w_gate, preferred_element_type=jnp.float32)
        up = jnp.dot(rows, w_up, preferred_element_type=jnp.float32)
        hidden = activate(gate, up)
        total = jnp.zeros((rows.shape[0], D), jnp.float32)
        for index in range(N_TP):
            part = jnp.dot(hidden[:, index * half:(index + 1) * half], w_down[index * half:(index + 1) * half], preferred_element_type=jnp.float32)
            part = lax.optimization_barrier(part.astype(jnp.bfloat16))
            total = total + part.astype(jnp.float32)
        return total.astype(jnp.bfloat16)
    results = lax.map(one_expert, (buffer, gate_proj, up_proj, down_proj)).reshape(-1, D)
    picked = results[target].reshape(TOKENS, TOP_K, D).astype(jnp.float32)
    mixed = lax.optimization_barrier(jnp.sum(picked * route_weights[:, :, None], axis=1))
    return norm_rows(mixed, post_gain).astype(jnp.bfloat16)
```

```python
import functools

import jax
import jax.numpy as jnp
from jax import lax
from jax.experimental import pallas as pl
from jax.experimental.pallas import tpu as pltpu
from jax.sharding import PartitionSpec as P

EPSILON = 1e-06
LIMIT = 7.0
ALPHA = 1.702
CHUNKS = 4
TILE = 256
PLANES = 4
MESH = pl.DeviceIdType.MESH


def activate(gate, up):
    gate = jnp.minimum(gate, LIMIT)
    up = jnp.clip(up, -LIMIT, LIMIT)
    return ((up + 1.0) * gate * jax.nn.sigmoid(ALPHA * gate)).astype(jnp.bfloat16)


def dot(a, b):
    return jnp.dot(a, b, preferred_element_type=jnp.float32)


def kernel(
    n, tps, cap,
    x_hbm, pre_ref, ids_ref, route_ref, gate_ref, up_ref, down_ref, post_ref, out_ref,
    x_ref, gate_v, up_v, down_v, held, meta, send, recv, ret,
    fp_send, fp_recv, mixed, hidden, places,
    x_sem, w_local, w_send, w_recv, n_send, n_recv, m_send, m_recv,
    d_send, d_recv, r_send, r_recv, q_send, q_recv,
):
    tokens, width = x_ref.shape
    pz = n // PLANES
    cw = width // CHUNKS
    rows = pz * cap
    fh = gate_v.shape[2]
    every = range(CHUNKS)
    me = lax.axis_index("ep")
    core = lax.axis_index("tp")
    plane = me // pz
    column = lax.rem(me, pz)
    inner = plane * (3 - plane) // 2
    outer = 1 - inner
    mine = outer
    mate_base = (plane + 1 - 2 * lax.rem(plane, 2)) * pz
    own_base = plane * pz
    mate = mate_base + column
    far = (3 - plane) * pz + column

    def on_inner(f):
        pl.when(inner == 1)(f)

    def on_outer(f):
        pl.when(inner == 0)(f)

    def ring(base, j):
        return base + lax.rem(column + j, pz)

    def greet(device):
        pl.semaphore_signal(barrier, inc=1, device_id=device, device_id_type=MESH)

    x_copy = pltpu.make_async_copy(x_hbm, x_ref, x_sem)
    x_copy.start()
    weights = ((gate_ref, gate_v), (up_ref, up_v), (down_ref, down_v))
    local_copies = [
        pltpu.make_async_copy(src.at[0], dst.at[core], w_local.at[w])
        for w, (src, dst) in enumerate(weights)
    ]
    for copy in local_copies:
        copy.start()

    barrier = pltpu.get_barrier_semaphore()

    @pl.loop(1, pz)
    def _(j):
        greet({"ep": ring(own_base, j)})

    @pl.loop(0, pz)
    def _(j):
        greet({"ep": ring(mate_base, j)})

    for i in range(1, tps):
        greet({"tp": lax.rem(core + i, tps)})

    @on_inner
    def _():
        greet({"ep": far})

    pl.semaphore_wait(barrier, 2 * pz - 1 + tps - 1 + inner)

    def remote(src, dst, ss, rs, where):
        return pltpu.make_async_remote_copy(
            src_ref=src, dst_ref=dst, send_sem=ss, recv_sem=rs,
            device_id=where, device_id_type=MESH,
        )

    def await_bytes(ref, sem):
        pltpu.make_async_copy(ref, ref, sem).wait()

    peer_copies = [
        [
            remote(
                src.at[0], dst.at[core], w_send.at[w, i - 1], w_recv.at[w, i - 1],
                {"tp": lax.rem(core + i, tps)},
            )
            for i in range(1, tps)
        ]
        for w, (src, dst) in enumerate(weights)
    ]
    for copies in peer_copies:
        for copy in copies:
            copy.start()

    meta[mine, 0:2, :] = ids_ref[...].astype(jnp.float32)
    meta[mine, 2:4, :] = route_ref[...]
    meta[mine, 4:8, :] = jnp.zeros((4, tokens), jnp.float32)

    def place(g, ts):
        values = meta[g]
        experts_col = lax.broadcasted_iota(jnp.int32, (n, 1), 0).astype(jnp.float32)
        earlier = (
            lax.broadcasted_iota(jnp.int32, (tokens, tokens), 0)
            < lax.broadcasted_iota(jnp.int32, (tokens, tokens), 1)
        ).astype(jnp.bfloat16)
        first, second = values[0:1, :], values[1:2, :]
        hot0 = (first == experts_col).astype(jnp.float32)
        hot1 = (second == experts_col).astype(jnp.float32)
        before = dot((hot0 + hot1).astype(jnp.bfloat16), earlier)
        for t in ts:
            start = (mate_base if t else own_base).astype(jnp.float32)
            places[2 * g + t] = values
            for i, (ids, hot) in enumerate(((first, hot0), (second, hot1))):
                slot = jnp.sum(before * hot, axis=0, keepdims=True)
                inside = (ids >= start) & (ids < start + pz)
                relative = ids - (start + column.astype(jnp.float32))
                relative = jnp.where(relative < 0, relative + pz, relative)
                places[2 * g + t, i : i + 1, :] = jnp.where(inside, relative * cap + slot, -1.0)

    def picker(k):
        at = lax.broadcasted_iota(jnp.int32, (rows, 1), 0).astype(jnp.float32)
        return (
            (places[k, 0:1, :] == at).astype(jnp.float32)
            + (places[k, 1:2, :] == at).astype(jnp.float32)
        ).astype(jnp.bfloat16)

    def mixer(k):
        columns = places[k].T
        at = lax.broadcasted_iota(jnp.int32, (1, rows), 1).astype(jnp.float32)
        w = jnp.where(columns[:, 0:1] == at, columns[:, 2:3], 0.0) + jnp.where(
            columns[:, 1:2] == at, columns[:, 3:4], 0.0
        )
        high = w.astype(jnp.bfloat16)
        return high, (w - high.astype(jnp.float32)).astype(jnp.bfloat16)

    def block_of(j):
        return pl.ds(pl.multiple_of(j * cap, cap), cap)

    def pick(g, t, c):
        k = 2 * g + t
        picked = dot(picker(k), held[g, c]).astype(jnp.bfloat16)
        if t == 0:
            recv[g, c, 0:cap, :] = picked[0:cap]
            send[k, c, cap:rows, :] = picked[cap:rows]
        else:
            send[k, c] = picked
        base = mate_base if t else own_base

        @pl.loop(1 - t, pz)
        def _(j):
            remote(
                send.at[k, c, block_of(j)], recv.at[g, c, block_of(j)],
                d_send.at[k, c], d_recv.at[g, c], {"ep": ring(base, j)},
            ).start()

    def received_in_plane(g):
        @pl.loop(0, CHUNKS)
        def _(c):
            await_bytes(recv.at[g, c, pl.ds(cap, rows - cap)], d_recv.at[g, c])

    def received_crossed(g):
        @pl.loop(0, CHUNKS)
        def _(c):
            await_bytes(recv.at[g, c], d_recv.at[g, c])

    def received(g):
        on_inner(lambda: received_in_plane(g))
        on_outer(lambda: received_crossed(g))

    def expand(g, i):
        h = lax.rem(core + i, tps)

        @pl.loop(0, fh // TILE)
        def _(t):
            at = pl.ds(pl.multiple_of(t * TILE, TILE), TILE)
            gate = jnp.zeros((rows, TILE), jnp.float32)
            up = jnp.zeros((rows, TILE), jnp.float32)
            for c in every:
                gate += dot(recv[g, c], gate_v[h, c * cw : (c + 1) * cw, at])
                up += dot(recv[g, c], up_v[h, c * cw : (c + 1) * cw, at])
            hidden[g, h, :, at] = activate(gate, up)

    def contract(g, t):
        k = 2 * g + t
        base = own_base + t * (mate_base - own_base)

        @pl.loop(0, CHUNKS)
        def _(c):
            for s in range(cw // TILE):
                lo = s * TILE
                total = jnp.zeros((rows, TILE), jnp.float32)
                for h in range(tps):
                    at = pl.ds(pl.multiple_of(c * cw + lo, TILE), TILE)
                    part = dot(hidden[g, h], down_v[h, :, at])
                    total += part.astype(jnp.bfloat16).astype(jnp.float32)
                recv[g, c, :, lo : lo + TILE] = total.astype(jnp.bfloat16)

            @pl.when(t == 0)
            def _():
                ret[k, c, 0:cap, :] = recv[g, c, 0:cap, :]

            @pl.loop(1 - t, pz)
            def _(j):
                remote(
                    recv.at[g, c, block_of(j)], ret.at[k, c, block_of(j)],
                    r_send.at[g, c], r_recv.at[k, c], {"ep": ring(base, pz - j)},
                ).start()

    def mix(g, t, c):
        k = 2 * g + t
        high, low = mixer(k)
        if t == 0:
            await_bytes(ret.at[k, c, pl.ds(cap, rows - cap)], r_recv.at[k, c])
        else:
            await_bytes(ret.at[k, c], r_recv.at[k, c])
        return dot(high, ret[k, c]) + dot(low, ret[k, c])

    x_copy.wait()
    squares = jnp.zeros((tokens, 1), jnp.float32)
    for c in every:
        xs = x_ref[:, c * cw : (c + 1) * cw].astype(jnp.float32)
        squares = squares + jnp.sum(xs * xs, axis=-1, keepdims=True)
    scale = lax.rsqrt(squares / width + EPSILON)
    partner = far * inner + mate * outer

    def rows_copy(step, c):
        if step == 0:
            return remote(
                held.at[mine, c], held.at[1 + inner, c], n_send.at[0, c], n_recv.at[1 + inner, c],
                {"ep": partner},
            )
        return remote(
            held.at[1, c], held.at[3, c], n_send.at[1, c], n_recv.at[3, c], {"ep": far}
        )

    def meta_copy(step):
        if step == 0:
            return remote(
                meta.at[mine], meta.at[1 + inner], m_send.at[0], m_recv.at[1 + inner],
                {"ep": partner},
            )
        return remote(meta.at[1], meta.at[3], m_send.at[1], m_recv.at[3], {"ep": far})

    def part_copy(kind, c):
        if kind == 2:
            return remote(
                fp_recv.at[1, c], fp_recv.at[1, c], q_send.at[2, c], q_recv.at[1, c], {"ep": mate}
            )
        return remote(
            fp_send.at[kind, c], fp_recv.at[kind, c], q_send.at[kind, c], q_recv.at[kind, c],
            {"ep": far},
        )

    def await_rows(g, c):
        await_bytes(held.at[g, c], n_recv.at[g, c])

    def await_meta(g):
        await_bytes(meta.at[g], m_recv.at[g])

    def await_part(kind, c):
        await_bytes(fp_recv.at[kind, c], q_recv.at[kind, c])

    def relay(c):
        await_rows(1, c)
        rows_copy(1, c).start()
        pick(1, 0, c)

    def accept(g, c):
        await_rows(g, c)
        pick(g, 1, c)
        pick(g, 0, c)

    def share(g, c):
        fp_send[g - 2, c] = (mix(g, 0, c) + mix(g, 1, c)).astype(jnp.bfloat16)
        part_copy(g - 2, c).start()

    meta_copy(0).start()
    for c in every:
        xs = x_ref[:, c * cw : (c + 1) * cw].astype(jnp.float32)
        held[mine, c] = (xs * scale * pre_ref[:, c * cw : (c + 1) * cw]).astype(jnp.bfloat16)
        if c == 0:
            rows_copy(0, c).start()
        else:
            on_outer(rows_copy(0, c).start)
    place(mine, (0, 1))

    @pl.loop(0, CHUNKS)
    def _(c):
        pick(mine, 0, c)
        on_inner(lambda: pick(0, 1, c))

    @on_inner
    def _():
        await_meta(1)
        meta_copy(1).start()
        place(1, (0,))

        @pl.loop(0, 2)
        def _(c):
            relay(c)

        await_meta(3)
        place(3, (0, 1))
        accept(3, 0)

    received_in_plane(mine)
    local_copies[0].wait()
    local_copies[1].wait()
    expand(mine, 0)

    @on_inner
    def _():
        await_meta(2)
        place(2, (0, 1))

        @pl.loop(2, CHUNKS)
        def _(c):
            relay(c)

            @pl.when(c == CHUNKS - 1)
            def _():
                for d in range(1, CHUNKS):
                    rows_copy(0, d).start()

            accept(3, c - 1)

    def await_peers(w):
        for copy in peer_copies[w]:
            copy.wait()

    on_outer(lambda: received_crossed(0))
    on_inner(lambda: await_peers(0))
    on_inner(lambda: await_peers(1))
    expand(0, inner)
    on_inner(lambda: received_in_plane(1))
    on_outer(lambda: await_peers(0))
    on_outer(lambda: await_peers(1))
    expand(inner, outer)

    @on_inner
    def _():
        accept(3, CHUNKS - 1)
        accept(2, 0)

    def await_down():
        local_copies[2].wait()
        await_peers(2)

    @on_outer
    def _():
        await_down()
        contract(0, 1)

    expand(1, 1)
    on_outer(lambda: contract(1, 0))
    received(3)
    expand(3, 0)
    on_inner(lambda: accept(2, 1))
    expand(3, 1)
    on_inner(await_down)
    contract(3, outer)

    @on_inner
    def _():
        @pl.loop(2, CHUNKS)
        def _(c):
            accept(2, c)

        @pl.loop(0, 2)
        def _(c):
            share(3, c)

        contract(1, 0)

    received(2)
    expand(2, 0)
    on_inner(lambda: share(3, 2))
    expand(2, 1)
    on_inner(lambda: share(3, 3))
    contract(2, outer)

    @on_inner
    def _():
        contract(0, 0)

        @pl.loop(0, CHUNKS)
        def _(c):
            value = mix(1, 0, c)
            await_part(1, c)
            fp_recv[1, c] = (value + fp_recv[1, c].astype(jnp.float32)).astype(jnp.bfloat16)
            part_copy(2, c).start()
            share(2, c)

    @pl.loop(0, CHUNKS)
    def _(c):
        mixed[c] = mix(mine, 0, c)

        @on_inner
        def _():
            mixed[c] = mixed[c] + mix(0, 1, c)

    squares = jnp.zeros((tokens, 1), jnp.float32)
    for c in every:
        await_part(mine, c)
        total = mixed[c] + fp_recv[mine, c].astype(jnp.float32)
        mixed[c] = total
        squares = squares + jnp.sum(total * total, axis=-1, keepdims=True)
    scale = lax.rsqrt(squares / width + EPSILON)
    for c in every:
        at = slice(c * cw, (c + 1) * cw)
        out_ref[:, at] = (mixed[c] * scale * post_ref[:, at]).astype(jnp.bfloat16)

    meta_copy(0).wait_send()
    on_inner(meta_copy(1).wait_send)

    @pl.loop(0, CHUNKS)
    def _(c):
        def in_plane(g):
            own = pl.ds(cap, rows - cap)
            await_bytes(send.at[2 * g, c, own], d_send.at[2 * g, c])
            await_bytes(recv.at[g, c, own], r_send.at[g, c])

        rows_copy(0, c).wait_send()
        in_plane(mine)

        @on_inner
        def _():
            rows_copy(1, c).wait_send()
            for kind in range(3):
                part_copy(kind, c).wait_send()
            for g in (1, 2, 3):
                in_plane(g)
            for g in (0, 2, 3):
                await_bytes(send.at[2 * g + 1, c], d_send.at[2 * g + 1, c])

        @on_outer
        def _():
            for g in (0, 2, 3):
                await_bytes(recv.at[g, c], r_send.at[g, c])


def local(inputs, pre_gain, expert_ids, route_weights, gate_proj, up_proj, down_proj, post_gain):
    tokens, width = inputs.shape
    choices = expert_ids.shape[1]
    n = lax.axis_size("ep")
    tps = lax.axis_size("tp")
    cap = 3 * tokens * choices // (2 * n * gate_proj.shape[0])
    cap = -(-cap // 16) * 16
    rows = n // PLANES * cap
    cw = width // CHUNKS
    fh = gate_proj.shape[2]
    bf16, f32 = jnp.bfloat16, jnp.float32
    vmem = pl.BlockSpec(memory_space=pltpu.VMEM)
    hbm = pl.BlockSpec(memory_space=pl.ANY)
    dma = pltpu.SemaphoreType.DMA
    return pl.pallas_call(
        functools.partial(kernel, n, tps, cap),
        out_shape=jax.ShapeDtypeStruct((tokens, width), bf16),
        in_specs=[hbm, vmem, vmem, vmem, hbm, hbm, hbm, vmem],
        out_specs=vmem,
        scratch_shapes=[
            pltpu.VMEM((tokens, width), bf16),
            pltpu.VMEM((tps, width, fh), bf16),
            pltpu.VMEM((tps, width, fh), bf16),
            pltpu.VMEM((tps, fh, width), bf16),
            pltpu.VMEM((4, CHUNKS, tokens, cw), bf16),
            pltpu.VMEM((4, 8, tokens), f32),
            pltpu.VMEM((8, CHUNKS, rows, cw), bf16),
            pltpu.VMEM((4, CHUNKS, rows, cw), bf16),
            pltpu.VMEM((8, CHUNKS, rows, cw), bf16),
            pltpu.VMEM((2, CHUNKS, tokens, cw), bf16),
            pltpu.VMEM((2, CHUNKS, tokens, cw), bf16),
            pltpu.VMEM((CHUNKS, tokens, cw), f32),
            pltpu.VMEM((4, tps, rows, fh), bf16),
            pltpu.VMEM((8, 8, tokens), f32),
            dma, dma((3,)), dma((3, tps - 1)), dma((3, tps - 1)),
            dma((2, CHUNKS)), dma((4, CHUNKS)), dma((2,)), dma((4,)),
            dma((8, CHUNKS)), dma((4, CHUNKS)), dma((4, CHUNKS)), dma((8, CHUNKS)),
            dma((3, CHUNKS)), dma((2, CHUNKS)),
        ],
        compiler_params=pltpu.CompilerParams(
            collective_id=0, has_side_effects=True, vmem_limit_bytes=67043328
        ),
    )(
        inputs, pre_gain[None, :], expert_ids.T, route_weights.T,
        gate_proj, up_proj, down_proj, post_gain[None, :],
    )


def solution(mesh):
    in_specs = (
        P(("ep", "tp"), None),
        P(),
        P(("ep", "tp"), None),
        P(("ep", "tp"), None),
        P("ep", None, "tp"),
        P("ep", None, "tp"),
        P("ep", "tp", None),
        P(),
    )
    out_specs = P(("ep", "tp"), None)
    return jax.shard_map(local, mesh=mesh, in_specs=in_specs, out_specs=out_specs, check_vma=False)
```

```python
import functools

import jax
import jax.numpy as jnp
from jax import lax
from jax.experimental import pallas as pl
from jax.experimental.pallas import tpu as pltpu
from jax.sharding import PartitionSpec as P

EPSILON = 1e-06
LIMIT = 7.0
ALPHA = 1.702
CHUNKS = 4
DIRECT = 2
TILE = 256
PLANES = 4
MESH = pl.DeviceIdType.MESH


def activate(gate, up):
    gate = jnp.minimum(gate, LIMIT)
    up = jnp.clip(up, -LIMIT, LIMIT)
    return ((up + 1.0) * gate * jax.nn.sigmoid(ALPHA * gate)).astype(jnp.bfloat16)


def dot(a, b):
    return jnp.dot(a, b, preferred_element_type=jnp.float32)


def kernel(
    n, tps, cap,
    x_hbm, pre_ref, ids_ref, route_ref, gate_ref, up_ref, down_ref, post_ref, out_hbm,
    x_ref, gate_v, up_v, down_v, held, meta, send, recv, ret,
    fp_send, fp_recv, mixed, hidden, places,
    x_sem, w_local, w_send, w_recv, n_send, n_recv, m_send, m_recv,
    d_send, d_recv, r_send, r_recv, f_send, q_send, q_recv, o_sem,
):
    tokens, width = x_ref.shape
    pz = n // PLANES
    cw = width // CHUNKS
    rows = pz * cap
    fh = gate_v.shape[2]
    every = range(CHUNKS)
    me = lax.axis_index("ep")
    core = lax.axis_index("tp")
    plane = me // pz
    column = lax.rem(me, pz)
    inner = plane * (3 - plane) // 2
    outer = 1 - inner
    mine = outer
    mate_base = (plane + 1 - 2 * lax.rem(plane, 2)) * pz
    own_base = plane * pz
    mate = mate_base + column
    far = (3 - plane) * pz + column

    def on_inner(f):
        pl.when(inner == 1)(f)

    def on_outer(f):
        pl.when(inner == 0)(f)

    def ring(base, j):
        return base + lax.rem(column + j, pz)

    def greet(device):
        pl.semaphore_signal(barrier, inc=1, device_id=device, device_id_type=MESH)

    x_copy = pltpu.make_async_copy(x_hbm, x_ref, x_sem)
    x_copy.start()
    weights = ((gate_ref, gate_v), (up_ref, up_v), (down_ref, down_v))
    local_copies = [
        pltpu.make_async_copy(src.at[0], dst.at[core], w_local.at[w])
        for w, (src, dst) in enumerate(weights)
    ]
    for copy in local_copies:
        copy.start()

    barrier = pltpu.get_barrier_semaphore()

    @pl.loop(1, pz)
    def _(j):
        greet({"ep": ring(own_base, j)})

    @pl.loop(0, pz)
    def _(j):
        greet({"ep": ring(mate_base, j)})

    for i in range(1, tps):
        greet({"tp": lax.rem(core + i, tps)})

    @on_inner
    def _():
        greet({"ep": far})

    def remote(src, dst, ss, rs, where):
        return pltpu.make_async_remote_copy(
            src_ref=src, dst_ref=dst, send_sem=ss, recv_sem=rs,
            device_id=where, device_id_type=MESH,
        )

    def await_bytes(ref, sem):
        pltpu.make_async_copy(ref, ref, sem).wait()

    peer_copies = [
        [
            remote(
                src.at[0], dst.at[core], w_send.at[w, i - 1], w_recv.at[w, i - 1],
                {"tp": lax.rem(core + i, tps)},
            )
            for i in range(1, tps)
        ]
        for w, (src, dst) in enumerate(weights)
    ]
    meta[mine, 0:2, :] = ids_ref[...].astype(jnp.float32)
    meta[mine, 2:4, :] = route_ref[...]
    meta[mine, 4:8, :] = jnp.zeros((4, tokens), jnp.float32)

    def place(g, ts):
        values = meta[g]
        experts_col = lax.broadcasted_iota(jnp.int32, (n, 1), 0).astype(jnp.float32)
        earlier = (
            lax.broadcasted_iota(jnp.int32, (tokens, tokens), 0)
            < lax.broadcasted_iota(jnp.int32, (tokens, tokens), 1)
        ).astype(jnp.bfloat16)
        first, second = values[0:1, :], values[1:2, :]
        hot0 = (first == experts_col).astype(jnp.float32)
        hot1 = (second == experts_col).astype(jnp.float32)
        before = dot((hot0 + hot1).astype(jnp.bfloat16), earlier)
        for t in ts:
            start = (mate_base if t else own_base).astype(jnp.float32)
            places[2 * g + t] = values
            for i, (ids, hot) in enumerate(((first, hot0), (second, hot1))):
                slot = jnp.sum(before * hot, axis=0, keepdims=True)
                inside = (ids >= start) & (ids < start + pz)
                relative = ids - (start + column.astype(jnp.float32))
                relative = jnp.where(relative < 0, relative + pz, relative)
                places[2 * g + t, i : i + 1, :] = jnp.where(inside, relative * cap + slot, -1.0)

    def picker(k):
        at = lax.broadcasted_iota(jnp.int32, (rows, 1), 0).astype(jnp.float32)
        return (
            (places[k, 0:1, :] == at).astype(jnp.float32)
            + (places[k, 1:2, :] == at).astype(jnp.float32)
        ).astype(jnp.bfloat16)

    def mixer(k):
        columns = places[k].T
        at = lax.broadcasted_iota(jnp.int32, (1, rows), 1).astype(jnp.float32)
        w = jnp.where(columns[:, 0:1] == at, columns[:, 2:3], 0.0) + jnp.where(
            columns[:, 1:2] == at, columns[:, 3:4], 0.0
        )
        high = w.astype(jnp.bfloat16)
        return high, (w - high.astype(jnp.float32)).astype(jnp.bfloat16)

    def block_of(j):
        return pl.ds(pl.multiple_of(j * cap, cap), cap)

    def pick(g, t, c):
        k = 2 * g + t
        picked = dot(picker(k), held[g, c]).astype(jnp.bfloat16)
        if t == 0:
            recv[g, c, 0:cap, :] = picked[0:cap]
            send[k, c, cap:rows, :] = picked[cap:rows]
        else:
            send[k, c] = picked
        base = mate_base if t else own_base

        @pl.loop(1 - t, pz)
        def _(j):
            remote(
                send.at[k, c, block_of(j)], recv.at[g, c, block_of(j)],
                d_send.at[k, c], d_recv.at[g, c], {"ep": ring(base, j)},
            ).start()

    def received_in_plane(g):
        @pl.loop(0, CHUNKS)
        def _(c):
            await_bytes(recv.at[g, c, pl.ds(cap, rows - cap)], d_recv.at[g, c])

    def received_crossed(g):
        @pl.loop(0, CHUNKS)
        def _(c):
            await_bytes(recv.at[g, c], d_recv.at[g, c])

    def received(g):
        on_inner(lambda: received_in_plane(g))
        on_outer(lambda: received_crossed(g))

    def expand(g, i):
        h = lax.rem(core + i, tps)

        @pl.loop(0, fh // TILE)
        def _(t):
            at = pl.ds(pl.multiple_of(t * TILE, TILE), TILE)
            gate = jnp.zeros((rows, TILE), jnp.float32)
            up = jnp.zeros((rows, TILE), jnp.float32)
            for c in every:
                gate += dot(recv[g, c], gate_v[h, c * cw : (c + 1) * cw, at])
                up += dot(recv[g, c], up_v[h, c * cw : (c + 1) * cw, at])
            hidden[g, h, :, at] = activate(gate, up)

    def contract(g, k, t, chunks=(0, CHUNKS)):
        base = own_base + t * (mate_base - own_base)

        @pl.loop(*chunks)
        def _(c):
            for s in range(cw // TILE):
                lo = s * TILE
                total = jnp.zeros((rows, TILE), jnp.float32)
                for h in range(tps):
                    at = pl.ds(pl.multiple_of(c * cw + lo, TILE), TILE)
                    part = dot(hidden[g, h], down_v[h, :, at])
                    total += part.astype(jnp.bfloat16).astype(jnp.float32)
                recv[g, c, :, lo : lo + TILE] = total.astype(jnp.bfloat16)

            @pl.when(t == 0)
            def _():
                ret[k, c, 0:cap, :] = recv[g, c, 0:cap, :]

            @pl.loop(1 - t, pz)
            def _(j):
                remote(
                    recv.at[g, c, block_of(j)], ret.at[k, c, block_of(j)],
                    r_send.at[g, c], r_recv.at[k, c], {"ep": ring(base, pz - j)},
                ).start()

    def mix(g, t, c):
        k = 2 * g + t
        high, low = mixer(k)
        if t == 0:
            await_bytes(ret.at[k, c, pl.ds(cap, rows - cap)], r_recv.at[k, c])
        else:
            await_bytes(ret.at[k, c], r_recv.at[k, c])
        return dot(high, ret[k, c]) + dot(low, ret[k, c])

    x_copy.wait()
    squares = jnp.zeros((tokens, 1), jnp.float32)
    for c in every:
        xs = x_ref[:, c * cw : (c + 1) * cw].astype(jnp.float32)
        squares = squares + jnp.sum(xs * xs, axis=-1, keepdims=True)
    scale = lax.rsqrt(squares / width + EPSILON)
    partner = far * inner + mate * outer

    def rows_copy(step, c):
        if step == 0:
            return remote(
                held.at[mine, c], held.at[1 + inner, c], n_send.at[0, c], n_recv.at[1 + inner, c],
                {"ep": partner},
            )
        return remote(
            held.at[1, c], held.at[3, c], n_send.at[1, c], n_recv.at[3, c], {"ep": far}
        )

    def meta_copy(step):
        if step == 0:
            return remote(
                meta.at[mine], meta.at[1 + inner], m_send.at[0], m_recv.at[1 + inner],
                {"ep": partner},
            )
        return remote(meta.at[1], meta.at[3], m_send.at[1], m_recv.at[3], {"ep": far})

    def part_copy(kind, c):
        if kind == 2:
            return remote(
                fp_recv.at[1, c], fp_recv.at[1, c], q_send.at[2, c], q_recv.at[1, c], {"ep": mate}
            )
        return remote(
            fp_send.at[kind, c], fp_recv.at[kind, c], q_send.at[kind, c], q_recv.at[kind, c],
            {"ep": far},
        )

    def await_rows(g, c):
        await_bytes(held.at[g, c], n_recv.at[g, c])

    def await_meta(g):
        await_bytes(meta.at[g], m_recv.at[g])

    def await_part(kind, c):
        await_bytes(fp_recv.at[kind, c], q_recv.at[kind, c])

    def relay(c):
        await_rows(1, c)
        rows_copy(1, c).start()
        pick(1, 0, c)

    def accept(g, c):
        await_rows(g, c)
        pick(g, 1, c)
        pick(g, 0, c)

    def forward_copy(g, c):
        k = 2 * g + 1
        return remote(
            ret.at[k, c], ret.at[k, c], f_send.at[g - 2, c], r_recv.at[k, c], {"ep": mate}
        )

    def forward(g, chunks):
        @pl.loop(*chunks)
        def _(c):
            k = 2 * g + 1
            await_bytes(ret.at[k, c, pl.ds(cap, rows - cap)], r_recv.at[k, c])
            forward_copy(g, c).start()

    def share(g, c):
        fp_send[g - 2, c] = (mix(g, 0, c) + mix(g, 1, c)).astype(jnp.bfloat16)
        part_copy(g - 2, c).start()

    for c in every:
        xs = x_ref[:, c * cw : (c + 1) * cw].astype(jnp.float32)
        held[mine, c] = (xs * scale * pre_ref[:, c * cw : (c + 1) * cw]).astype(jnp.bfloat16)
    place(mine, (0, 1))
    pl.semaphore_wait(barrier, 2 * pz - 1 + tps - 1 + inner)
    meta_copy(0).start()
    rows_copy(0, 0).start()
    for c in range(1, CHUNKS):
        on_outer(rows_copy(0, c).start)
    for copies in peer_copies:
        for copy in copies:
            copy.start()

    @pl.loop(0, CHUNKS)
    def _(c):
        pick(mine, 0, c)
        on_inner(lambda: pick(0, 1, c))

    @on_inner
    def _():
        await_meta(1)
        meta_copy(1).start()
        place(1, (0,))

        @pl.loop(0, 2)
        def _(c):
            relay(c)

        await_meta(3)
        place(3, (0, 1))
        accept(3, 0)

    received_in_plane(mine)
    local_copies[0].wait()
    local_copies[1].wait()
    expand(mine, 0)

    @on_inner
    def _():
        await_meta(2)
        place(2, (0, 1))

        @pl.loop(2, CHUNKS)
        def _(c):
            relay(c)

            @pl.when(c == CHUNKS - 1)
            def _():
                for d in range(1, CHUNKS):
                    rows_copy(0, d).start()

            accept(3, c - 1)

    def await_peers(w):
        for copy in peer_copies[w]:
            copy.wait()

    on_outer(lambda: received_crossed(0))
    on_inner(lambda: await_peers(0))
    on_inner(lambda: await_peers(1))
    expand(0, inner)
    on_inner(lambda: received_in_plane(1))
    on_outer(lambda: await_peers(0))
    on_outer(lambda: await_peers(1))
    expand(inner, outer)

    @on_inner
    def _():
        accept(3, CHUNKS - 1)
        accept(2, 0)

    def await_down():
        local_copies[2].wait()
        await_peers(2)

    @on_outer
    def _():
        await_down()
        contract(0, 1, 1)

    expand(1, 1)
    on_outer(lambda: contract(1, 2, 0))
    received(3)
    expand(3, 0)
    on_inner(lambda: accept(2, 1))
    expand(3, 1)
    on_inner(await_down)
    contract(3, 6 + outer, outer, (0, DIRECT))
    on_inner(lambda: accept(2, 2))

    @on_outer
    def _():
        contract(3, 7, 0, (DIRECT, CHUNKS))
        forward(3, (DIRECT, CHUNKS))

    @on_inner
    def _():
        accept(2, 3)
        share(3, 0)
        contract(3, 6, 0, (DIRECT, CHUNKS))
        share(3, 1)
        contract(1, 3, 1)

    received(2)
    expand(2, 0)
    on_inner(lambda: share(3, 2))
    expand(2, 1)
    on_inner(lambda: share(3, 3))
    contract(2, 4 + outer, 0)
    on_outer(lambda: forward(2, (0, CHUNKS)))

    @on_inner
    def _():
        contract(0, 0, 0)

        @pl.loop(0, CHUNKS)
        def _(c):
            await_part(1, c)
            part_copy(2, c).start()
            share(2, c)

    @pl.loop(0, CHUNKS)
    def _(c):
        mixed[c] = mix(mine, 0, c) + mix(mine, 1, c)

    def out_copy(c):
        at = pl.ds(c * cw, cw)
        return pltpu.make_async_copy(x_ref.at[:, at], out_hbm.at[:, at], o_sem.at[c])

    squares = jnp.zeros((tokens, 1), jnp.float32)
    for c in every:
        await_part(mine, c)
        total = mixed[c] + fp_recv[mine, c].astype(jnp.float32)
        mixed[c] = total
        squares = squares + jnp.sum(total * total, axis=-1, keepdims=True)
    scale = lax.rsqrt(squares / width + EPSILON)
    for c in every:
        at = slice(c * cw, (c + 1) * cw)
        x_ref[:, at] = (mixed[c] * scale * post_ref[:, at]).astype(jnp.bfloat16)
        out_copy(c).start()

    meta_copy(0).wait_send()
    on_inner(meta_copy(1).wait_send)

    @pl.loop(0, CHUNKS)
    def _(c):
        def in_plane(g):
            own = pl.ds(cap, rows - cap)
            await_bytes(recv.at[g, c, own], r_send.at[g, c])

        def picked(g):
            own = pl.ds(cap, rows - cap)
            await_bytes(send.at[2 * g, c, own], d_send.at[2 * g, c])

        rows_copy(0, c).wait_send()
        picked(mine)
        in_plane(mine)

        @on_inner
        def _():
            rows_copy(1, c).wait_send()
            for kind in range(3):
                part_copy(kind, c).wait_send()
            for g in (1, 2, 3):
                picked(g)
            for g in (2, 3):
                in_plane(g)
            await_bytes(recv.at[1, c], r_send.at[1, c])
            for g in (0, 2, 3):
                await_bytes(send.at[2 * g + 1, c], d_send.at[2 * g + 1, c])

        @on_outer
        def _():
            await_bytes(recv.at[0, c], r_send.at[0, c])
            in_plane(2)
            forward_copy(2, c).wait_send()

            @pl.when(c < DIRECT)
            def _():
                await_bytes(recv.at[3, c], r_send.at[3, c])

            @pl.when(c >= DIRECT)
            def _():
                in_plane(3)
                forward_copy(3, c).wait_send()

    for c in every:
        out_copy(c).wait()


def local(inputs, pre_gain, expert_ids, route_weights, gate_proj, up_proj, down_proj, post_gain):
    tokens, width = inputs.shape
    choices = expert_ids.shape[1]
    n = lax.axis_size("ep")
    tps = lax.axis_size("tp")
    cap = 3 * tokens * choices // (2 * n * gate_proj.shape[0])
    cap = -(-cap // 16) * 16
    rows = n // PLANES * cap
    cw = width // CHUNKS
    fh = gate_proj.shape[2]
    bf16, f32 = jnp.bfloat16, jnp.float32
    vmem = pl.BlockSpec(memory_space=pltpu.VMEM)
    hbm = pl.BlockSpec(memory_space=pl.ANY)
    dma = pltpu.SemaphoreType.DMA
    return pl.pallas_call(
        functools.partial(kernel, n, tps, cap),
        out_shape=jax.ShapeDtypeStruct((tokens, width), bf16),
        in_specs=[hbm, vmem, vmem, vmem, hbm, hbm, hbm, vmem],
        out_specs=hbm,
        scratch_shapes=[
            pltpu.VMEM((tokens, width), bf16),
            pltpu.VMEM((tps, width, fh), bf16),
            pltpu.VMEM((tps, width, fh), bf16),
            pltpu.VMEM((tps, fh, width), bf16),
            pltpu.VMEM((4, CHUNKS, tokens, cw), bf16),
            pltpu.VMEM((4, 8, tokens), f32),
            pltpu.VMEM((8, CHUNKS, rows, cw), bf16),
            pltpu.VMEM((4, CHUNKS, rows, cw), bf16),
            pltpu.VMEM((8, CHUNKS, rows, cw), bf16),
            pltpu.VMEM((2, CHUNKS, tokens, cw), bf16),
            pltpu.VMEM((2, CHUNKS, tokens, cw), bf16),
            pltpu.VMEM((CHUNKS, tokens, cw), f32),
            pltpu.VMEM((4, tps, rows, fh), bf16),
            pltpu.VMEM((8, 8, tokens), f32),
            dma, dma((3,)), dma((3, tps - 1)), dma((3, tps - 1)),
            dma((2, CHUNKS)), dma((4, CHUNKS)), dma((2,)), dma((4,)),
            dma((8, CHUNKS)), dma((4, CHUNKS)), dma((4, CHUNKS)), dma((8, CHUNKS)),
            dma((2, CHUNKS)), dma((3, CHUNKS)), dma((2, CHUNKS)), dma((CHUNKS,)),
        ],
        compiler_params=pltpu.CompilerParams(
            collective_id=0, has_side_effects=True, vmem_limit_bytes=67043328
        ),
    )(
        inputs, pre_gain[None, :], expert_ids.T, route_weights.T,
        gate_proj, up_proj, down_proj, post_gain[None, :],
    )


def solution(mesh):
    in_specs = (
        P(("ep", "tp"), None),
        P(),
        P(("ep", "tp"), None),
        P(("ep", "tp"), None),
        P("ep", None, "tp"),
        P("ep", None, "tp"),
        P("ep", "tp", None),
        P(),
    )
    out_specs = P(("ep", "tp"), None)
    return jax.shard_map(local, mesh=mesh, in_specs=in_specs, out_specs=out_specs, check_vma=False)
```

```python
import functools

import jax
import jax.numpy as jnp
from jax import lax
from jax.experimental import pallas as pl
from jax.experimental.pallas import tpu as pltpu
from jax.sharding import PartitionSpec as P

EPSILON = 1e-06
LIMIT = 7.0
ALPHA = 1.702
CHUNKS = 8
DIRECT = 4
EARLY = 2
LATER = 6
BLOCKS = 4
PAIR = 2
TILE = 256
PLANES = 4
MESH = pl.DeviceIdType.MESH


def activate(gate, up):
    gate = jnp.minimum(gate, LIMIT)
    up = jnp.clip(up, -LIMIT, LIMIT)
    return ((up + 1.0) * gate * jax.nn.sigmoid(ALPHA * gate)).astype(jnp.bfloat16)


def dot(a, b):
    return jnp.dot(a, b, preferred_element_type=jnp.float32)


def kernel(
    n, tps, cap,
    x_hbm, pre_ref, ids_ref, route_ref, gate_ref, up_ref, down_ref, post_ref, out_hbm,
    x_ref, gate_v, up_v, down_v, held, meta, send, recv, ret,
    fp_send, fp_recv, mixed, hidden, places, mixers,
    x_sem, w_local, w_send, w_recv, n_send, n_recv, m_send, m_recv,
    d_send, d_recv, r_send, r_near, r_recv, f_send, q_send, q_recv, o_sem,
):
    tokens, width = x_ref.shape
    pz = n // PLANES
    cw = width // CHUNKS
    rows = pz * cap
    fh = gate_v.shape[2]
    every = range(CHUNKS)
    me = lax.axis_index("ep")
    core = lax.axis_index("tp")
    plane = me // pz
    column = lax.rem(me, pz)
    inner = plane * (3 - plane) // 2
    outer = 1 - inner
    mine = outer
    mate_base = (plane + 1 - 2 * lax.rem(plane, 2)) * pz
    own_base = plane * pz
    mate = mate_base + column
    far = (3 - plane) * pz + column

    def on_inner(f):
        pl.when(inner == 1)(f)

    def on_outer(f):
        pl.when(inner == 0)(f)

    def ring(base, j):
        return base + lax.rem(column + j, pz)

    def greet(device):
        pl.semaphore_signal(barrier, inc=1, device_id=device, device_id_type=MESH)

    x_copy = pltpu.make_async_copy(x_hbm, x_ref, x_sem)
    x_copy.start()
    weights = ((gate_ref, gate_v), (up_ref, up_v), (down_ref, down_v))
    local_copies = [
        pltpu.make_async_copy(src.at[0], dst.at[core], w_local.at[w])
        for w, (src, dst) in enumerate(weights)
    ]
    for copy in local_copies:
        copy.start()

    barrier = pltpu.get_barrier_semaphore()

    @pl.loop(1, pz)
    def _(j):
        greet({"ep": ring(own_base, j)})

    @pl.loop(0, pz)
    def _(j):
        greet({"ep": ring(mate_base, j)})

    for i in range(1, tps):
        greet({"tp": lax.rem(core + i, tps)})

    @on_inner
    def _():
        greet({"ep": far})

    def remote(src, dst, ss, rs, where):
        return pltpu.make_async_remote_copy(
            src_ref=src, dst_ref=dst, send_sem=ss, recv_sem=rs,
            device_id=where, device_id_type=MESH,
        )

    def await_bytes(ref, sem):
        pltpu.make_async_copy(ref, ref, sem).wait()

    peer_copies = [
        [
            remote(
                src.at[0], dst.at[core], w_send.at[w, i - 1], w_recv.at[w, i - 1],
                {"tp": lax.rem(core + i, tps)},
            )
            for i in range(1, tps)
        ]
        for w, (src, dst) in enumerate(weights)
    ]
    meta[mine, 0:2, :] = ids_ref[...].astype(jnp.float32)
    meta[mine, 2:4, :] = route_ref[...]
    meta[mine, 4:8, :] = jnp.zeros((4, tokens), jnp.float32)

    def place(g, ts):
        values = meta[g]
        experts_col = lax.broadcasted_iota(jnp.int32, (n, 1), 0).astype(jnp.float32)
        earlier = (
            lax.broadcasted_iota(jnp.int32, (tokens, tokens), 0)
            < lax.broadcasted_iota(jnp.int32, (tokens, tokens), 1)
        ).astype(jnp.bfloat16)
        first, second = values[0:1, :], values[1:2, :]
        hot0 = (first == experts_col).astype(jnp.float32)
        hot1 = (second == experts_col).astype(jnp.float32)
        before = dot((hot0 + hot1).astype(jnp.bfloat16), earlier)
        for t in ts:
            start = (mate_base if t else own_base).astype(jnp.float32)
            places[2 * g + t] = values
            for i, (ids, hot) in enumerate(((first, hot0), (second, hot1))):
                slot = jnp.sum(before * hot, axis=0, keepdims=True)
                inside = (ids >= start) & (ids < start + pz)
                relative = ids - (start + column.astype(jnp.float32))
                relative = jnp.where(relative < 0, relative + pz, relative)
                places[2 * g + t, i : i + 1, :] = jnp.where(inside, relative * cap + slot, -1.0)

    def picker(k):
        at = lax.broadcasted_iota(jnp.int32, (rows, 1), 0).astype(jnp.float32)
        return (
            (places[k, 0:1, :] == at).astype(jnp.float32)
            + (places[k, 1:2, :] == at).astype(jnp.float32)
        ).astype(jnp.bfloat16)

    def prepare(k):
        columns = places[k].T
        at = lax.broadcasted_iota(jnp.int32, (1, rows), 1).astype(jnp.float32)
        w = jnp.where(columns[:, 0:1] == at, columns[:, 2:3], 0.0) + jnp.where(
            columns[:, 1:2] == at, columns[:, 3:4], 0.0
        )
        high = w.astype(jnp.bfloat16)
        mixers[k, 0] = high
        mixers[k, 1] = (w - high.astype(jnp.float32)).astype(jnp.bfloat16)

    def block_of(j):
        return pl.ds(pl.multiple_of(j * cap, cap), cap)

    def pick(g, t, c):
        k = 2 * g + t
        picked = dot(picker(k), held[g, c]).astype(jnp.bfloat16)
        if t == 0:
            recv[g, c, 0:cap, :] = picked[0:cap]
            send[k, c, cap:rows, :] = picked[cap:rows]
        else:
            send[k, c] = picked
        base = mate_base if t else own_base

        @pl.loop(1 - t, pz)
        def _(j):
            remote(
                send.at[k, c, block_of(j)], recv.at[g, c, block_of(j)],
                d_send.at[k], d_recv.at[g], {"ep": ring(base, j)},
            ).start()

    def received_in_plane(g):
        await_bytes(recv.at[g, :, pl.ds(cap, rows - cap)], d_recv.at[g])

    def received_crossed(g):
        await_bytes(recv.at[g], d_recv.at[g])

    def received(g):
        on_inner(lambda: received_in_plane(g))
        on_outer(lambda: received_crossed(g))

    def expand(g, i, first=0, tiles=fh // TILE):
        h = lax.rem(core + i, tps)

        @pl.loop(first, first + tiles)
        def _(t):
            at = pl.ds(pl.multiple_of(t * TILE, TILE), TILE)
            gate = jnp.zeros((rows, TILE), jnp.float32)
            up = jnp.zeros((rows, TILE), jnp.float32)
            for c in every:
                gate += dot(recv[g, c], gate_v[h, c * cw : (c + 1) * cw, at])
                up += dot(recv[g, c], up_v[h, c * cw : (c + 1) * cw, at])
            hidden[g, h, :, at] = activate(gate, up)

    def came(g, k, c):
        return r_near.at[k] if isinstance(g, int) and g < 2 else r_recv.at[k - 4, c]

    def contract(g, k, t, chunks=(0, CHUNKS)):
        base = own_base + t * (mate_base - own_base)

        @pl.loop(chunks[0] // PAIR, chunks[1] // PAIR)
        def _(p):
            total = jnp.zeros((rows, PAIR * cw), jnp.float32)
            for h in range(tps):
                at = pl.ds(pl.multiple_of(p * PAIR * cw, PAIR * cw), PAIR * cw)
                part = dot(hidden[g, h], down_v[h, :, at])
                total += part.astype(jnp.bfloat16).astype(jnp.float32)
            total = total.astype(jnp.bfloat16)
            for q in range(PAIR):
                recv[g, PAIR * p + q] = total[:, q * cw : (q + 1) * cw]

            @pl.when(t == 0)
            def _():
                for q in range(PAIR):
                    ret[k, PAIR * p + q, 0:cap, :] = total[0:cap, q * cw : (q + 1) * cw]

            for q in range(PAIR):
                c = PAIR * p + q

                @pl.loop(1 - t, pz)
                def _(j):
                    remote(
                        recv.at[g, c, block_of(j)], ret.at[k, c, block_of(j)],
                        r_send.at[g], came(g, k, c), {"ep": ring(base, pz - j)},
                    ).start()

    def mix(k, c):
        return dot(mixers[k, 0], ret[k, c]) + dot(mixers[k, 1], ret[k, c])

    def await_far(g, t, c):
        k = 2 * g + t
        part = ret.at[k, c] if t else ret.at[k, c, pl.ds(cap, rows - cap)]
        await_bytes(part, came(g, k, c))

    x_copy.wait()
    squares = jnp.zeros((tokens, 1), jnp.float32)
    for c in every:
        xs = x_ref[:, c * cw : (c + 1) * cw].astype(jnp.float32)
        squares = squares + jnp.sum(xs * xs, axis=-1, keepdims=True)
    scale = lax.rsqrt(squares / width + EPSILON)
    partner = far * inner + mate * outer

    def rows_copy(step, c):
        if step == 0:
            return remote(
                held.at[mine, c], held.at[1 + inner, c], n_send.at[0], n_recv.at[inner, c],
                {"ep": partner},
            )
        return remote(
            held.at[1, c], held.at[3, c], n_send.at[1], n_recv.at[2, c], {"ep": far}
        )

    def meta_copy(step):
        if step == 0:
            return remote(
                meta.at[mine], meta.at[1 + inner], m_send.at[0], m_recv.at[1 + inner],
                {"ep": partner},
            )
        return remote(meta.at[1], meta.at[3], m_send.at[1], m_recv.at[3], {"ep": far})

    def part_copy(kind, c):
        if kind == 2:
            return remote(
                fp_recv.at[1, c], fp_recv.at[1, c], q_send.at[2], q_recv.at[1, c], {"ep": mate}
            )
        return remote(
            fp_send.at[kind, c], fp_recv.at[kind, c], q_send.at[kind], q_recv.at[kind, c],
            {"ep": far},
        )

    def await_rows(g, c):
        await_bytes(held.at[g, c], n_recv.at[g - 1, c])

    def await_meta(g):
        await_bytes(meta.at[g], m_recv.at[g])

    def await_part(kind, c):
        await_bytes(fp_recv.at[kind, c], q_recv.at[kind, c])

    def relay(c):
        await_rows(1, c)
        rows_copy(1, c).start()
        pick(1, 0, c)

    def accept(g, c):
        await_rows(g, c)
        pick(g, 1, c)
        pick(g, 0, c)

    def forward_copy(g, c):
        k = 2 * g + 1
        return remote(
            ret.at[k, c], ret.at[k, c], f_send.at[g - 2], came(g, k, c), {"ep": mate}
        )

    def forward(g, chunks):
        @pl.loop(*chunks)
        def _(c):
            k = 2 * g + 1
            await_bytes(ret.at[k, c, pl.ds(cap, rows - cap)], came(g, k, c))
            forward_copy(g, c).start()

    def share(g, c):
        await_far(g, 0, c)
        await_far(g, 1, c)
        fp_send[g - 2, c] = (mix(2 * g, c) + mix(2 * g + 1, c)).astype(jnp.bfloat16)
        part_copy(g - 2, c).start()

    for c in every:
        xs = x_ref[:, c * cw : (c + 1) * cw].astype(jnp.float32)
        held[mine, c] = (xs * scale * pre_ref[:, c * cw : (c + 1) * cw]).astype(jnp.bfloat16)
    place(mine, (0, 1))
    pl.semaphore_wait(barrier, 2 * pz - 1 + tps - 1 + inner)
    def await_peers(w):
        for copy in peer_copies[w]:
            copy.wait()

    meta_copy(0).start()

    @pl.loop(0, outer * CHUNKS + inner * EARLY)
    def _(c):
        rows_copy(0, c).start()

    for copies in peer_copies:
        for copy in copies:
            copy.start()

    @pl.loop(0, CHUNKS)
    def _(c):
        pick(mine, 0, c)
        on_inner(lambda: pick(0, 1, c))

    @on_inner
    def _():
        await_meta(1)
        meta_copy(1).start()
        place(1, (0,))

        @pl.loop(0, 3)
        def _(c):
            relay(c)

        await_meta(3)
        place(3, (0, 1))
        accept(3, 0)
        relay(3)
        accept(3, 1)
        received_in_plane(0)
        local_copies[0].wait()
        local_copies[1].wait()
        await_meta(2)
        place(2, (0, 1))
        some = tps * (fh // TILE) // (CHUNKS - 4)

        @pl.loop(4, CHUNKS)
        def _(c):
            relay(c)

            @pl.when(c == CHUNKS - 1)
            def _():
                @pl.loop(EARLY, CHUNKS)
                def _(d):
                    rows_copy(0, d).start()

            accept(3, c - 2)

            @pl.when(c == CHUNKS - 2)
            def _():
                await_peers(0)
                await_peers(1)

            tile = (c - 4) * some
            expand(0, tile // (fh // TILE), lax.rem(tile, fh // TILE), some)

    def accept_all(g, chunks):
        @pl.loop(*chunks)
        def _(c):
            accept(g, c)

    def share_all(g, chunks):
        @pl.loop(*chunks)
        def _(c):
            share(g, c)

    def pass_on(c):
        await_part(1, c)
        part_copy(2, c).start()

    def await_down():
        local_copies[2].wait()
        await_peers(2)

    @on_inner
    def _():
        accept_all(3, (CHUNKS - 2, CHUNKS))
        accept_all(2, (0, EARLY))
        received_in_plane(1)
        expand(1, 0)

    @on_outer
    def _():
        received_crossed(0)
        local_copies[0].wait()
        local_copies[1].wait()
        expand(0, 0)
        await_peers(0)
        await_peers(1)
        for i in range(1, tps):
            expand(0, i)
        await_down()
        contract(0, 1, 1)
        received_in_plane(1)
        for i in range(tps):
            expand(1, i)

    received(3)
    expand(3, 0)
    on_inner(lambda: accept_all(2, (2, 4)))
    expand(3, 1)
    on_inner(await_down)
    contract(3, 6 + outer, outer, (0, DIRECT))

    @on_outer
    def _():
        contract(3, 7, 0, (DIRECT, CHUNKS))
        forward(3, (DIRECT, LATER))

    @on_inner
    def _():
        accept_all(2, (4, 6))
        prepare(6)
        prepare(7)
        accept(2, 6)
        share(3, 0)
        accept(2, 7)
        share(3, 1)
        expand(1, 1)
        contract(1, 3, 1, (0, 4))
        share(3, 2)
        contract(3, 6, 0, (DIRECT, CHUNKS))
        share(3, 3)
        contract(1, 3, 1, (4, CHUNKS))
        prepare(4)
        prepare(5)

    received(2)
    expand(2, 0)
    on_inner(lambda: share_all(3, (4, 6)))
    on_outer(lambda: forward(3, (LATER, CHUNKS)))
    expand(2, 1)
    on_inner(lambda: share_all(3, (6, CHUNKS)))
    contract(2, 4 + outer, 0)

    @on_outer
    def _():
        forward(2, (0, CHUNKS))
        contract(1, 2, 0)


    @on_inner
    def _():
        @pl.loop(0, 4)
        def _(c):
            pass_on(c)

        share_all(2, (0, 2))
        contract(0, 0, 0)

        @pl.loop(2, CHUNKS)
        def _(c):
            share(2, c)
            pl.when(c < CHUNKS - 2)(lambda: pass_on(c + 2))

    prepare(2 * mine)
    prepare(2 * mine + 1)
    await_bytes(ret.at[2 * mine, :, pl.ds(cap, rows - cap)], r_near.at[2 * mine])
    await_bytes(ret.at[2 * mine + 1], r_near.at[2 * mine + 1])

    @pl.loop(0, CHUNKS)
    def _(c):
        mixed[c] = mix(2 * mine, c) + mix(2 * mine + 1, c)

    meta_copy(0).wait_send()
    on_inner(meta_copy(1).wait_send)
    others = pl.ds(cap, rows - cap)

    def picked(g):
        await_bytes(send.at[2 * g, :, others], d_send.at[2 * g])

    def in_plane(g):
        await_bytes(recv.at[g, :, others], r_send.at[g])

    picked(mine)
    in_plane(mine)

    @on_inner
    def _():
        await_bytes(held.at[0], n_send.at[0])
        await_bytes(held.at[1], n_send.at[1])
        for g in (1, 2, 3):
            picked(g)
        for g in (2, 3):
            in_plane(g)
        await_bytes(recv.at[1], r_send.at[1])
        for g in (0, 2, 3):
            await_bytes(send.at[2 * g + 1], d_send.at[2 * g + 1])
        for kind in range(2):
            await_bytes(fp_send.at[kind], q_send.at[kind])

    @on_outer
    def _():
        await_bytes(held.at[1], n_send.at[0])
        await_bytes(recv.at[0], r_send.at[0])
        in_plane(2)
        await_bytes(ret.at[5], f_send.at[0])
        some = pl.ds(DIRECT, CHUNKS - DIRECT)
        await_bytes(recv.at[3, pl.ds(0, DIRECT)], r_send.at[3])
        await_bytes(recv.at[3, some, others], r_send.at[3])
        await_bytes(ret.at[7, some], f_send.at[1])

    def out_copy(b):
        at = pl.ds(b * (tokens // BLOCKS), tokens // BLOCKS)
        return pltpu.make_async_copy(x_ref.at[at], out_hbm.at[at], o_sem.at[b])

    squares = jnp.zeros((tokens, 1), jnp.float32)
    for c in every:
        await_part(mine, c)
        total = mixed[c] + fp_recv[mine, c].astype(jnp.float32)
        mixed[c] = total
        squares = squares + jnp.sum(total * total, axis=-1, keepdims=True)
    scale = lax.rsqrt(squares / width + EPSILON)
    for b in range(BLOCKS):
        own = slice(b * (tokens // BLOCKS), (b + 1) * (tokens // BLOCKS))
        for c in every:
            at = slice(c * cw, (c + 1) * cw)
            x_ref[own, at] = (mixed[c, own] * scale[own] * post_ref[:, at]).astype(jnp.bfloat16)
        out_copy(b).start()

    on_inner(lambda: await_bytes(fp_recv.at[1], q_send.at[2]))

    for b in range(BLOCKS):
        out_copy(b).wait()


def local(inputs, pre_gain, expert_ids, route_weights, gate_proj, up_proj, down_proj, post_gain):
    tokens, width = inputs.shape
    choices = expert_ids.shape[1]
    n = lax.axis_size("ep")
    tps = lax.axis_size("tp")
    cap = 3 * tokens * choices // (2 * n * gate_proj.shape[0])
    cap = -(-cap // 16) * 16
    rows = n // PLANES * cap
    cw = width // CHUNKS
    fh = gate_proj.shape[2]
    bf16, f32 = jnp.bfloat16, jnp.float32
    vmem = pl.BlockSpec(memory_space=pltpu.VMEM)
    hbm = pl.BlockSpec(memory_space=pl.ANY)
    dma = pltpu.SemaphoreType.DMA
    return pl.pallas_call(
        functools.partial(kernel, n, tps, cap),
        out_shape=jax.ShapeDtypeStruct((tokens, width), bf16),
        in_specs=[hbm, vmem, vmem, vmem, hbm, hbm, hbm, vmem],
        out_specs=hbm,
        scratch_shapes=[
            pltpu.VMEM((tokens, width), bf16),
            pltpu.VMEM((tps, width, fh), bf16),
            pltpu.VMEM((tps, width, fh), bf16),
            pltpu.VMEM((tps, fh, width), bf16),
            pltpu.VMEM((4, CHUNKS, tokens, cw), bf16),
            pltpu.VMEM((4, 8, tokens), f32),
            pltpu.VMEM((8, CHUNKS, rows, cw), bf16),
            pltpu.VMEM((4, CHUNKS, rows, cw), bf16),
            pltpu.VMEM((8, CHUNKS, rows, cw), bf16),
            pltpu.VMEM((2, CHUNKS, tokens, cw), bf16),
            pltpu.VMEM((2, CHUNKS, tokens, cw), bf16),
            pltpu.VMEM((CHUNKS, tokens, cw), f32),
            pltpu.VMEM((4, tps, rows, fh), bf16),
            pltpu.VMEM((8, 8, tokens), f32),
            pltpu.VMEM((8, 2, tokens, rows), bf16),
            dma, dma((3,)), dma((3, tps - 1)), dma((3, tps - 1)),
            dma((2,)), dma((3, CHUNKS)), dma((2,)), dma((4,)),
            dma((8,)), dma((4,)), dma((4,)), dma((4,)), dma((4, CHUNKS)),
            dma((2,)), dma((3,)), dma((2, CHUNKS)), dma((BLOCKS,)),
        ],
        compiler_params=pltpu.CompilerParams(
            collective_id=0, has_side_effects=True, vmem_limit_bytes=67043328
        ),
    )(
        inputs, pre_gain[None, :], expert_ids.T, route_weights.T,
        gate_proj, up_proj, down_proj, post_gain[None, :],
    )


def solution(mesh):
    in_specs = (
        P(("ep", "tp"), None),
        P(),
        P(("ep", "tp"), None),
        P(("ep", "tp"), None),
        P("ep", None, "tp"),
        P("ep", None, "tp"),
        P("ep", "tp", None),
        P(),
    )
    out_specs = P(("ep", "tp"), None)
    return jax.shard_map(local, mesh=mesh, in_specs=in_specs, out_specs=out_specs, check_vma=False)
```

```python
import functools

import jax
import jax.numpy as jnp
from jax import lax
from jax.experimental import pallas as pl
from jax.experimental.pallas import tpu as pltpu
from jax.sharding import PartitionSpec as P

EPSILON = 1e-06
LIMIT = 7.0
ALPHA = 1.702
CHUNKS = 8
DIRECT = 4
EARLY = 2
SPLIT = 6
LATER = 6
BLOCKS = 4
PAIR = 2
TILE = 256
PLANES = 4
MESH = pl.DeviceIdType.MESH


def activate(gate, up):
    gate = jnp.minimum(gate, LIMIT)
    up = jnp.clip(up, -LIMIT, LIMIT)
    return ((up + 1.0) * gate * jax.nn.sigmoid(ALPHA * gate)).astype(jnp.bfloat16)


def dot(a, b):
    return jnp.dot(a, b, preferred_element_type=jnp.float32)


def kernel(
    n, tps, cap,
    x_hbm, pre_ref, ids_ref, route_ref, gate_ref, up_ref, down_ref, post_ref, out_ref,
    gate_v, up_v, down_v, held, meta, send, recv, ret,
    fp_send, fp_recv, acc, hidden, places, mixers,
    x_sem, w_local, w_send, w_recv, n_send, n_recv, m_send, m_recv,
    d_send, d_recv, r_send, r_near, r_recv, f_send, q_send, q_recv,
):
    tokens, width = out_ref.shape
    pz = n // PLANES
    cw = width // CHUNKS
    rows = pz * cap
    fh = gate_v.shape[2]
    every = range(CHUNKS)
    me = lax.axis_index("ep")
    core = lax.axis_index("tp")
    plane = me // pz
    column = lax.rem(me, pz)
    inner = plane * (3 - plane) // 2
    outer = 1 - inner
    mine = outer
    mate_base = (plane + 1 - 2 * lax.rem(plane, 2)) * pz
    own_base = plane * pz
    mate = mate_base + column
    far = (3 - plane) * pz + column

    def on_inner(f):
        pl.when(inner == 1)(f)

    def on_outer(f):
        pl.when(inner == 0)(f)

    def ring(base, j):
        return base + lax.rem(column + j, pz)

    def greet(device):
        pl.semaphore_signal(barrier, inc=1, device_id=device, device_id_type=MESH)

    x_copy = pltpu.make_async_copy(x_hbm, out_ref, x_sem)
    x_copy.start()
    weights = ((gate_ref, gate_v), (up_ref, up_v), (down_ref, down_v))
    local_copies = [
        pltpu.make_async_copy(src.at[0], dst.at[core], w_local.at[w])
        for w, (src, dst) in enumerate(weights)
    ]
    for copy in local_copies:
        copy.start()

    barrier = pltpu.get_barrier_semaphore()

    @pl.loop(1, pz)
    def _(j):
        greet({"ep": ring(own_base, j)})

    @pl.loop(0, pz)
    def _(j):
        greet({"ep": ring(mate_base, j)})

    for i in range(1, tps):
        greet({"tp": lax.rem(core + i, tps)})

    @on_inner
    def _():
        greet({"ep": far})

    def remote(src, dst, ss, rs, where):
        return pltpu.make_async_remote_copy(
            src_ref=src, dst_ref=dst, send_sem=ss, recv_sem=rs,
            device_id=where, device_id_type=MESH,
        )

    def await_bytes(ref, sem):
        pltpu.make_async_copy(ref, ref, sem).wait()

    peer_copies = [
        [
            remote(
                src.at[0], dst.at[core], w_send.at[w, i - 1], w_recv.at[w, i - 1],
                {"tp": lax.rem(core + i, tps)},
            )
            for i in range(1, tps)
        ]
        for w, (src, dst) in enumerate(weights)
    ]
    meta[mine, 0:2, :] = ids_ref[...].astype(jnp.float32)
    meta[mine, 2:4, :] = route_ref[...]
    meta[mine, 4:8, :] = jnp.zeros((4, tokens), jnp.float32)

    def place(g, ts):
        values = meta[g]
        experts_col = lax.broadcasted_iota(jnp.int32, (n, 1), 0).astype(jnp.float32)
        earlier = (
            lax.broadcasted_iota(jnp.int32, (tokens, tokens), 0)
            < lax.broadcasted_iota(jnp.int32, (tokens, tokens), 1)
        ).astype(jnp.bfloat16)
        first, second = values[0:1, :], values[1:2, :]
        hot0 = (first == experts_col).astype(jnp.float32)
        hot1 = (second == experts_col).astype(jnp.float32)
        before = dot((hot0 + hot1).astype(jnp.bfloat16), earlier)
        for t in ts:
            start = (mate_base if t else own_base).astype(jnp.float32)
            places[2 * g + t] = values
            for i, (ids, hot) in enumerate(((first, hot0), (second, hot1))):
                slot = jnp.sum(before * hot, axis=0, keepdims=True)
                inside = (ids >= start) & (ids < start + pz)
                relative = ids - (start + column.astype(jnp.float32))
                relative = jnp.where(relative < 0, relative + pz, relative)
                places[2 * g + t, i : i + 1, :] = jnp.where(inside, relative * cap + slot, -1.0)

    def picker(k):
        at = lax.broadcasted_iota(jnp.int32, (rows, 1), 0).astype(jnp.float32)
        return (
            (places[k, 0:1, :] == at).astype(jnp.float32)
            + (places[k, 1:2, :] == at).astype(jnp.float32)
        ).astype(jnp.bfloat16)

    def prepare(k, r):
        columns = places[k].T
        at = lax.broadcasted_iota(jnp.int32, (1, rows), 1).astype(jnp.float32)
        w = jnp.where(columns[:, 0:1] == at, columns[:, 2:3], 0.0) + jnp.where(
            columns[:, 1:2] == at, columns[:, 3:4], 0.0
        )
        high = w.astype(jnp.bfloat16)
        mixers[r, 0] = high
        mixers[r, 1] = (w - high.astype(jnp.float32)).astype(jnp.bfloat16)

    def block_of(j):
        return pl.ds(pl.multiple_of(j * cap, cap), cap)

    def sent(g, t):
        return 2 * g + t - (1 if isinstance(g, int) and g > 1 else 0)

    def pick(g, t, c):
        k = sent(g, t)
        picked = dot(picker(2 * g + t), held[g, c]).astype(jnp.bfloat16)
        if t == 0:
            recv[g, c, 0:cap, :] = picked[0:cap]
            send[k, c, cap:rows, :] = picked[cap:rows]
        else:
            send[k, c] = picked
        base = mate_base if t else own_base
        late = c // SPLIT if isinstance(g, int) and g == 3 else 0

        @pl.loop(1 - t, pz)
        def _(j):
            remote(
                send.at[k, c, block_of(j)], recv.at[g, c, block_of(j)],
                d_send.at[k], d_recv.at[g + late], {"ep": ring(base, j)},
            ).start()

    def received_in_plane(g):
        await_bytes(recv.at[g, :, pl.ds(cap, rows - cap)], d_recv.at[g])

    def received_crossed(g):
        await_bytes(recv.at[g], d_recv.at[g])

    def received(g):
        on_inner(lambda: received_in_plane(g))
        on_outer(lambda: received_crossed(g))

    def received_part(late):
        part = pl.ds(SPLIT * late, SPLIT + late * (CHUNKS - 2 * SPLIT))
        on_inner(lambda: await_bytes(recv.at[3, part, pl.ds(cap, rows - cap)], d_recv.at[3 + late]))
        on_outer(lambda: await_bytes(recv.at[3, part], d_recv.at[3 + late]))

    def begin(i):
        h = lax.rem(core + i, tps)

        @pl.loop(0, fh // TILE)
        def _(t):
            at = pl.ds(pl.multiple_of(t * TILE, TILE), TILE)
            gate = jnp.zeros((rows, TILE), jnp.float32)
            up = jnp.zeros((rows, TILE), jnp.float32)
            for c in range(SPLIT):
                gate += dot(recv[3, c], gate_v[h, c * cw : (c + 1) * cw, at])
                up += dot(recv[3, c], up_v[h, c * cw : (c + 1) * cw, at])
            acc[2 * i, 0:rows, at] = gate
            acc[2 * i + 1, 0:rows, at] = up

    def complete(i):
        h = lax.rem(core + i, tps)

        @pl.loop(0, fh // TILE)
        def _(t):
            at = pl.ds(pl.multiple_of(t * TILE, TILE), TILE)
            gate = jnp.zeros((rows, TILE), jnp.float32)
            up = jnp.zeros((rows, TILE), jnp.float32)
            for c in range(SPLIT, CHUNKS):
                gate += dot(recv[3, c], gate_v[h, c * cw : (c + 1) * cw, at])
                up += dot(recv[3, c], up_v[h, c * cw : (c + 1) * cw, at])
            gate += acc[2 * i, 0:rows, at]
            up += acc[2 * i + 1, 0:rows, at]
            hidden[3, h, :, at] = activate(gate, up)

    def expand(g, i, first=0, tiles=fh // TILE):
        h = lax.rem(core + i, tps)

        @pl.loop(first, first + tiles)
        def _(t):
            at = pl.ds(pl.multiple_of(t * TILE, TILE), TILE)
            gate = jnp.zeros((rows, TILE), jnp.float32)
            up = jnp.zeros((rows, TILE), jnp.float32)
            for c in every:
                gate += dot(recv[g, c], gate_v[h, c * cw : (c + 1) * cw, at])
                up += dot(recv[g, c], up_v[h, c * cw : (c + 1) * cw, at])
            hidden[g, h, :, at] = activate(gate, up)

    def came(g, k, c):
        return r_near.at[k] if g < 2 else r_recv.at[k - 2, c]

    def contract(g, k, t, chunks=(0, CHUNKS)):
        base = own_base + t * (mate_base - own_base)

        @pl.loop(chunks[0] // PAIR, chunks[1] // PAIR)
        def _(p):
            total = jnp.zeros((rows, PAIR * cw), jnp.float32)
            for h in range(tps):
                at = pl.ds(pl.multiple_of(p * PAIR * cw, PAIR * cw), PAIR * cw)
                part = dot(hidden[g, h], down_v[h, :, at])
                total += part.astype(jnp.bfloat16).astype(jnp.float32)
            total = total.astype(jnp.bfloat16)
            for q in range(PAIR):
                recv[g, PAIR * p + q] = total[:, q * cw : (q + 1) * cw]

            @pl.when(t == 0)
            def _():
                for q in range(PAIR):
                    ret[k, PAIR * p + q, 0:cap, :] = total[0:cap, q * cw : (q + 1) * cw]

            for q in range(PAIR):
                c = PAIR * p + q

                @pl.loop(1 - t, pz)
                def _(j):
                    remote(
                        recv.at[g, c, block_of(j)], ret.at[k, c, block_of(j)],
                        r_send.at[g], came(g, k, c), {"ep": ring(base, pz - j)},
                    ).start()

    def mix(k, c):
        return dot(mixers[k, 0], ret[k, c]) + dot(mixers[k, 1], ret[k, c])

    def await_far(g, t, c):
        k = 2 * g - 2 + t
        part = ret.at[k, c] if t else ret.at[k, c, pl.ds(cap, rows - cap)]
        await_bytes(part, came(g, k, c))

    x_copy.wait()
    squares = jnp.zeros((tokens, 1), jnp.float32)
    for c in every:
        xs = out_ref[:, c * cw : (c + 1) * cw].astype(jnp.float32)
        squares = squares + jnp.sum(xs * xs, axis=-1, keepdims=True)
    scale = lax.rsqrt(squares / width + EPSILON)
    partner = far * inner + mate * outer

    def rows_copy(step, c):
        if step == 0:
            return remote(
                held.at[mine, c], held.at[1 + inner, c], n_send.at[0], n_recv.at[inner, c],
                {"ep": partner},
            )
        return remote(
            held.at[1, c], held.at[3, c], n_send.at[1], n_recv.at[2, c], {"ep": far}
        )

    def meta_copy(step):
        if step == 0:
            return remote(
                meta.at[mine], meta.at[1 + inner], m_send.at[0], m_recv.at[1 + inner],
                {"ep": partner},
            )
        return remote(meta.at[1], meta.at[3], m_send.at[1], m_recv.at[3], {"ep": far})

    def part_copy(kind, c):
        if kind == 2:
            return remote(
                fp_recv.at[1, c], fp_recv.at[1, c], q_send.at[2], q_recv.at[1, c], {"ep": mate}
            )
        return remote(
            fp_send.at[kind, c], fp_recv.at[kind, c], q_send.at[kind], q_recv.at[kind, c],
            {"ep": far},
        )

    def await_rows(g, c):
        await_bytes(held.at[g, c], n_recv.at[g - 1, c])

    def await_meta(g):
        await_bytes(meta.at[g], m_recv.at[g])

    def await_part(kind, c):
        await_bytes(fp_recv.at[kind, c], q_recv.at[kind, c])

    def relay(c):
        await_rows(1, c)
        rows_copy(1, c).start()
        pick(1, 0, c)

    def accept(g, c):
        await_rows(g, c)
        pick(g, 1, c)
        pick(g, 0, c)

    def forward_copy(g, c):
        k = 2 * g - 1
        return remote(
            ret.at[k, c], ret.at[k, c], f_send.at[g - 2], came(g, k, c), {"ep": mate}
        )

    def forward(g, chunks):
        @pl.loop(*chunks)
        def _(c):
            k = 2 * g - 1
            await_bytes(ret.at[k, c, pl.ds(cap, rows - cap)], came(g, k, c))
            forward_copy(g, c).start()

    def share(g, c):
        await_far(g, 0, c)
        await_far(g, 1, c)
        fp_send[g - 2, c] = (mix(2 * g - 2, c) + mix(2 * g - 1, c)).astype(jnp.bfloat16)
        part_copy(g - 2, c).start()

    for c in every:
        xs = out_ref[:, c * cw : (c + 1) * cw].astype(jnp.float32)
        held[mine, c] = (xs * scale * pre_ref[:, c * cw : (c + 1) * cw]).astype(jnp.bfloat16)
    place(mine, (0, 1))
    pl.semaphore_wait(barrier, 2 * pz - 1 + tps - 1 + inner)
    def await_peers(w):
        for copy in peer_copies[w]:
            copy.wait()

    meta_copy(0).start()

    @pl.loop(0, outer * CHUNKS + inner * EARLY)
    def _(c):
        rows_copy(0, c).start()

    for copies in peer_copies:
        for copy in copies:
            copy.start()

    @pl.loop(0, CHUNKS)
    def _(c):
        pick(mine, 0, c)
        on_inner(lambda: pick(0, 1, c))

    @on_inner
    def _():
        await_meta(1)
        meta_copy(1).start()
        place(1, (0,))

        @pl.loop(0, 3)
        def _(c):
            relay(c)

        await_meta(3)
        place(3, (0, 1))
        accept(3, 0)
        relay(3)
        accept(3, 1)
        received_in_plane(0)
        local_copies[0].wait()
        local_copies[1].wait()
        await_meta(2)
        place(2, (0, 1))
        some = tps * (fh // TILE) // (CHUNKS - 4)

        @pl.loop(4, CHUNKS)
        def _(c):
            relay(c)

            @pl.when(c == CHUNKS - 1)
            def _():
                @pl.loop(EARLY, CHUNKS)
                def _(d):
                    rows_copy(0, d).start()

            accept(3, c - 2)

            @pl.when(c == CHUNKS - 2)
            def _():
                await_peers(0)
                await_peers(1)

            tile = (c - 4) * some
            expand(0, tile // (fh // TILE), lax.rem(tile, fh // TILE), some)

    def accept_all(g, chunks):
        @pl.loop(*chunks)
        def _(c):
            accept(g, c)

    def share_all(g, chunks):
        @pl.loop(*chunks)
        def _(c):
            share(g, c)

    def pass_on(c):
        await_part(1, c)
        part_copy(2, c).start()

    def await_down():
        local_copies[2].wait()
        await_peers(2)

    @on_inner
    def _():
        accept(3, CHUNKS - 2)
        prepare(6, 4)
        prepare(7, 5)
        accept(3, CHUNKS - 1)
        accept_all(2, (0, EARLY))

    @on_outer
    def _():
        received_crossed(0)
        local_copies[0].wait()
        local_copies[1].wait()
        expand(0, 0)
        await_peers(0)
        await_peers(1)
        for i in range(1, tps):
            expand(0, i)
        await_down()
        contract(0, 1, 1, (0, LATER))

    received_part(0)
    begin(0)
    on_inner(lambda: accept(2, 2))
    begin(1)
    on_inner(lambda: accept(2, 3))
    on_inner(await_down)
    received_part(1)
    for i in range(tps):
        complete(i)
    contract(3, 4 + outer, outer, (0, DIRECT))

    @on_outer
    def _():
        contract(3, 5, 0, (DIRECT, CHUNKS))
        received_in_plane(1)
        expand(1, 0)
        forward(3, (DIRECT, LATER))
        contract(0, 1, 1, (LATER, CHUNKS))
        expand(1, 1)

    @on_inner
    def _():
        accept_all(2, (4, 6))
        received_in_plane(1)
        expand(1, 0)
        accept(2, 6)
        share(3, 0)
        expand(1, 1, 0, fh // TILE // 2)
        accept(2, 7)
        expand(1, 1, fh // TILE // 2, fh // TILE // 2)
        share(3, 1)
        contract(1, 1, 1, (0, 4))
        share(3, 2)
        contract(3, 4, 0, (DIRECT, CHUNKS))
        share(3, 3)
        contract(1, 1, 1, (4, CHUNKS))
        prepare(4, 2)
        prepare(5, 3)

    received(2)
    expand(2, 0)
    on_inner(lambda: share_all(3, (4, 6)))
    on_outer(lambda: forward(3, (LATER, CHUNKS)))
    expand(2, 1)
    on_inner(lambda: share_all(3, (6, CHUNKS)))
    contract(2, 2 + outer, outer, (0, PAIR))
    contract(2, 2 + outer, 0, (PAIR, CHUNKS))

    @on_outer
    def _():
        forward(2, (PAIR, CHUNKS))
        contract(1, 0, 0)


    @on_inner
    def _():
        @pl.loop(0, 4)
        def _(c):
            pass_on(c)

        share_all(2, (0, 2))
        contract(0, 0, 0)

        @pl.loop(2, CHUNKS)
        def _(c):
            share(2, c)
            pl.when(c < CHUNKS - 2)(lambda: pass_on(c + 2))

    def mixed(c):
        per = fh // cw
        at = pl.ds(pl.multiple_of(lax.rem(c, per) * cw, cw), cw)
        return acc.at[c // per, pl.ds(0, tokens), at]

    prepare(2 * mine, 0)
    prepare(2 * mine + 1, 1)
    await_bytes(ret.at[0, :, pl.ds(cap, rows - cap)], r_near.at[0])
    await_bytes(ret.at[1], r_near.at[1])

    @pl.loop(0, CHUNKS)
    def _(c):
        mixed(c)[...] = mix(0, c) + mix(1, c)

    meta_copy(0).wait_send()
    on_inner(meta_copy(1).wait_send)
    others = pl.ds(cap, rows - cap)

    def picked(g):
        await_bytes(send.at[sent(g, 0), :, others], d_send.at[sent(g, 0)])

    def in_plane(g):
        await_bytes(recv.at[g, :, others], r_send.at[g])

    picked(mine)
    in_plane(mine)

    @on_inner
    def _():
        await_bytes(held.at[0], n_send.at[0])
        await_bytes(held.at[1], n_send.at[1])
        for g in (1, 2, 3):
            picked(g)
        for g in (2, 3):
            in_plane(g)
        await_bytes(recv.at[1], r_send.at[1])
        for g in (0, 2, 3):
            await_bytes(send.at[sent(g, 1)], d_send.at[sent(g, 1)])
        for kind in range(2):
            await_bytes(fp_send.at[kind], q_send.at[kind])

    @on_outer
    def _():
        await_bytes(held.at[1], n_send.at[0])
        await_bytes(recv.at[0], r_send.at[0])
        for g, direct in ((2, PAIR), (3, DIRECT)):
            some = pl.ds(direct, CHUNKS - direct)
            await_bytes(recv.at[g, pl.ds(0, direct)], r_send.at[g])
            await_bytes(recv.at[g, some, others], r_send.at[g])
            await_bytes(ret.at[2 * g - 1, some], f_send.at[g - 2])

    squares = jnp.zeros((tokens, 1), jnp.float32)
    for c in every:
        await_part(mine, c)
        total = mixed(c)[...] + fp_recv[mine, c].astype(jnp.float32)
        mixed(c)[...] = total
        squares = squares + jnp.sum(total * total, axis=-1, keepdims=True)
    scale = lax.rsqrt(squares / width + EPSILON)
    for c in every:
        at = slice(c * cw, (c + 1) * cw)
        out_ref[:, at] = (mixed(c)[...] * scale * post_ref[:, at]).astype(jnp.bfloat16)

    on_inner(lambda: await_bytes(fp_recv.at[1], q_send.at[2]))


def local(inputs, pre_gain, expert_ids, route_weights, gate_proj, up_proj, down_proj, post_gain):
    tokens, width = inputs.shape
    choices = expert_ids.shape[1]
    n = lax.axis_size("ep")
    tps = lax.axis_size("tp")
    cap = 3 * tokens * choices // (2 * n * gate_proj.shape[0])
    cap = -(-cap // 16) * 16
    rows = n // PLANES * cap
    cw = width // CHUNKS
    fh = gate_proj.shape[2]
    bf16, f32 = jnp.bfloat16, jnp.float32
    vmem = pl.BlockSpec(memory_space=pltpu.VMEM)
    hbm = pl.BlockSpec(memory_space=pltpu.HBM)
    dma = pltpu.SemaphoreType.DMA
    return pl.pallas_call(
        functools.partial(kernel, n, tps, cap),
        out_shape=pltpu.VMEM((tokens, width), bf16),
        in_specs=[hbm, vmem, vmem, vmem, hbm, hbm, hbm, vmem],
        out_specs=vmem,
        scratch_shapes=[
            pltpu.VMEM((tps, width, fh), bf16),
            pltpu.VMEM((tps, width, fh), bf16),
            pltpu.VMEM((tps, fh, width), bf16),
            pltpu.VMEM((4, CHUNKS, tokens, cw), bf16),
            pltpu.VMEM((4, 8, tokens), f32),
            pltpu.VMEM((7, CHUNKS, rows, cw), bf16),
            pltpu.VMEM((4, CHUNKS, rows, cw), bf16),
            pltpu.VMEM((6, CHUNKS, rows, cw), bf16),
            pltpu.VMEM((2, CHUNKS, tokens, cw), bf16),
            pltpu.VMEM((2, CHUNKS, tokens, cw), bf16),
            pltpu.VMEM((2 * tps, max(rows, tokens), fh), f32),
            pltpu.VMEM((4, tps, rows, fh), bf16),
            pltpu.VMEM((8, 8, tokens), f32),
            pltpu.VMEM((6, 2, tokens, rows), bf16),
            dma, dma((3,)), dma((3, tps - 1)), dma((3, tps - 1)),
            dma((2,)), dma((3, CHUNKS)), dma((2,)), dma((4,)),
            dma((7,)), dma((5,)), dma((4,)), dma((2,)), dma((4, CHUNKS)),
            dma((2,)), dma((3,)), dma((2, CHUNKS)),
        ],
        compiler_params=pltpu.CompilerParams(
            collective_id=0, has_side_effects=True, vmem_limit_bytes=67043328 - 2**20
        ),
    )(
        inputs, pre_gain[None, :], expert_ids.T, route_weights.T,
        gate_proj, up_proj, down_proj, post_gain[None, :],
    )


def solution(mesh):
    in_specs = (
        P(("ep", "tp"), None),
        P(),
        P(("ep", "tp"), None),
        P(("ep", "tp"), None),
        P("ep", None, "tp"),
        P("ep", None, "tp"),
        P("ep", "tp", None),
        P(),
    )
    out_specs = P(("ep", "tp"), None)
    return jax.shard_map(local, mesh=mesh, in_specs=in_specs, out_specs=out_specs, check_vma=False)
```

```python
import functools

import jax
import jax.numpy as jnp
from jax import lax
from jax.experimental import pallas as pl
from jax.experimental.pallas import tpu as pltpu
from jax.sharding import PartitionSpec as P

EPSILON = 1e-06
LIMIT = 7.0
ALPHA = 1.702
CHUNKS = 8
DIRECT = 4
EARLY = 2
SPLIT = 6
STRAIGHT = 6
LATER = 6
BLOCKS = 4
PAIR = 2
TILE = 256
PLANES = 4
MESH = pl.DeviceIdType.MESH


def activate(gate, up):
    gate = jnp.minimum(gate, LIMIT)
    up = jnp.clip(up, -LIMIT, LIMIT)
    return ((up + 1.0) * gate * jax.nn.sigmoid(ALPHA * gate)).astype(jnp.bfloat16)


def dot(a, b):
    return jnp.dot(a, b, preferred_element_type=jnp.float32)


def kernel(
    n, tps, cap,
    x_hbm, pre_hbm, ids_hbm, route_hbm, gate_ref, up_ref, down_ref, post_hbm, out_ref,
    pre_ref, ids_ref, route_ref, post_ref, gate_v, up_v, down_v, held, meta, send, recv, ret,
    fp_send, fp_recv, acc, hidden, places, mixers,
    x_sem, s_sem, w_local, w_send, w_recv, n_send, n_recv, m_send, m_recv,
    d_send, d_recv, r_send, r_near, r_recv, f_send, q_send, q_recv,
):
    tokens, width = out_ref.shape
    pz = n // PLANES
    cw = width // CHUNKS
    rows = pz * cap
    fh = gate_v.shape[2]
    every = range(CHUNKS)
    me = lax.axis_index("ep")
    core = lax.axis_index("tp")
    plane = me // pz
    column = lax.rem(me, pz)
    inner = plane * (3 - plane) // 2
    outer = 1 - inner
    mine = outer
    mate_base = (plane + 1 - 2 * lax.rem(plane, 2)) * pz
    own_base = plane * pz
    mate = mate_base + column
    far = (3 - plane) * pz + column

    def on_inner(f):
        pl.when(inner == 1)(f)

    def on_outer(f):
        pl.when(inner == 0)(f)

    def ring(base, j):
        return base + lax.rem(column + j, pz)

    def greet(device):
        pl.semaphore_signal(barrier, inc=1, device_id=device, device_id_type=MESH)

    x_copy = pltpu.make_async_copy(x_hbm, out_ref, x_sem)
    x_copy.start()
    small_copies = [
        pltpu.make_async_copy(src, dst, s_sem.at[i])
        for i, (src, dst) in enumerate(
            ((pre_hbm, pre_ref), (ids_hbm, ids_ref), (route_hbm, route_ref), (post_hbm, post_ref))
        )
    ]
    for copy in small_copies:
        copy.start()
    weights = ((gate_ref, gate_v), (up_ref, up_v), (down_ref, down_v))
    local_copies = [
        pltpu.make_async_copy(src.at[0], dst.at[core], w_local.at[w])
        for w, (src, dst) in enumerate(weights)
    ]
    barrier = pltpu.get_barrier_semaphore()

    @pl.loop(1, pz)
    def _(j):
        greet({"ep": ring(own_base, j)})

    @pl.loop(0, pz)
    def _(j):
        greet({"ep": ring(mate_base, j)})

    for i in range(1, tps):
        greet({"tp": lax.rem(core + i, tps)})

    @on_inner
    def _():
        greet({"ep": far})

    def remote(src, dst, ss, rs, where):
        return pltpu.make_async_remote_copy(
            src_ref=src, dst_ref=dst, send_sem=ss, recv_sem=rs,
            device_id=where, device_id_type=MESH,
        )

    def await_bytes(ref, sem):
        pltpu.make_async_copy(ref, ref, sem).wait()

    peer_copies = [
        [
            remote(
                src.at[0], dst.at[core], w_send.at[w, i - 1], w_recv.at[w, i - 1],
                {"tp": lax.rem(core + i, tps)},
            )
            for i in range(1, tps)
        ]
        for w, (src, dst) in enumerate(weights)
    ]
    def place(g, ts):
        values = meta[g]
        experts_col = lax.broadcasted_iota(jnp.int32, (n, 1), 0).astype(jnp.float32)
        earlier = (
            lax.broadcasted_iota(jnp.int32, (tokens, tokens), 0)
            < lax.broadcasted_iota(jnp.int32, (tokens, tokens), 1)
        ).astype(jnp.bfloat16)
        first, second = values[0:1, :], values[1:2, :]
        hot0 = (first == experts_col).astype(jnp.float32)
        hot1 = (second == experts_col).astype(jnp.float32)
        before = dot((hot0 + hot1).astype(jnp.bfloat16), earlier)
        for t in ts:
            start = (mate_base if t else own_base).astype(jnp.float32)
            places[2 * g + t] = values
            for i, (ids, hot) in enumerate(((first, hot0), (second, hot1))):
                slot = jnp.sum(before * hot, axis=0, keepdims=True)
                inside = (ids >= start) & (ids < start + pz)
                relative = ids - (start + column.astype(jnp.float32))
                relative = jnp.where(relative < 0, relative + pz, relative)
                places[2 * g + t, i : i + 1, :] = jnp.where(inside, relative * cap + slot, -1.0)

    def picker(k):
        at = lax.broadcasted_iota(jnp.int32, (rows, 1), 0).astype(jnp.float32)
        return (
            (places[k, 0:1, :] == at).astype(jnp.float32)
            + (places[k, 1:2, :] == at).astype(jnp.float32)
        ).astype(jnp.bfloat16)

    def prepare(k, r):
        columns = places[k].T
        at = lax.broadcasted_iota(jnp.int32, (1, rows), 1).astype(jnp.float32)
        w = jnp.where(columns[:, 0:1] == at, columns[:, 2:3], 0.0) + jnp.where(
            columns[:, 1:2] == at, columns[:, 3:4], 0.0
        )
        high = w.astype(jnp.bfloat16)
        mixers[r, 0] = high
        mixers[r, 1] = (w - high.astype(jnp.float32)).astype(jnp.bfloat16)

    def block_of(j):
        return pl.ds(pl.multiple_of(j * cap, cap), cap)

    def sent(g, t):
        return 2 * g + t - (1 if isinstance(g, int) and g > 1 else 0)

    def pick(g, t, c):
        k = sent(g, t)
        picked = dot(picker(2 * g + t), held[g, c]).astype(jnp.bfloat16)
        if t == 0:
            recv[g, c, 0:cap, :] = picked[0:cap]
            send[k, c, cap:rows, :] = picked[cap:rows]
        else:
            send[k, c] = picked
        base = mate_base if t else own_base
        late = c // SPLIT if isinstance(g, int) and g == 3 else 0

        @pl.loop(1 - t, pz)
        def _(j):
            remote(
                send.at[k, c, block_of(j)], recv.at[g, c, block_of(j)],
                d_send.at[k], d_recv.at[g + late], {"ep": ring(base, j)},
            ).start()

    def received_in_plane(g):
        await_bytes(recv.at[g, :, pl.ds(cap, rows - cap)], d_recv.at[g])

    def received_crossed(g):
        await_bytes(recv.at[g], d_recv.at[g])

    def received(g):
        on_inner(lambda: received_in_plane(g))
        on_outer(lambda: received_crossed(g))

    def received_part(late):
        part = pl.ds(SPLIT * late, SPLIT + late * (CHUNKS - 2 * SPLIT))
        on_inner(lambda: await_bytes(recv.at[3, part, pl.ds(cap, rows - cap)], d_recv.at[3 + late]))
        on_outer(lambda: await_bytes(recv.at[3, part], d_recv.at[3 + late]))

    def begin(i):
        h = lax.rem(core + i, tps)

        @pl.loop(0, fh // TILE)
        def _(t):
            at = pl.ds(pl.multiple_of(t * TILE, TILE), TILE)
            gate = jnp.zeros((rows, TILE), jnp.float32)
            up = jnp.zeros((rows, TILE), jnp.float32)
            for c in range(SPLIT):
                gate += dot(recv[3, c], gate_v[h, c * cw : (c + 1) * cw, at])
                up += dot(recv[3, c], up_v[h, c * cw : (c + 1) * cw, at])
            acc[2 * i, 0:rows, at] = gate
            acc[2 * i + 1, 0:rows, at] = up

    def complete(i):
        h = lax.rem(core + i, tps)

        @pl.loop(0, fh // TILE)
        def _(t):
            at = pl.ds(pl.multiple_of(t * TILE, TILE), TILE)
            gate = jnp.zeros((rows, TILE), jnp.float32)
            up = jnp.zeros((rows, TILE), jnp.float32)
            for c in range(SPLIT, CHUNKS):
                gate += dot(recv[3, c], gate_v[h, c * cw : (c + 1) * cw, at])
                up += dot(recv[3, c], up_v[h, c * cw : (c + 1) * cw, at])
            gate += acc[2 * i, 0:rows, at]
            up += acc[2 * i + 1, 0:rows, at]
            hidden[3, h, :, at] = activate(gate, up)

    def expand(g, i, first=0, tiles=fh // TILE):
        h = lax.rem(core + i, tps)

        @pl.loop(first, first + tiles)
        def _(t):
            at = pl.ds(pl.multiple_of(t * TILE, TILE), TILE)
            gate = jnp.zeros((rows, TILE), jnp.float32)
            up = jnp.zeros((rows, TILE), jnp.float32)
            for c in every:
                gate += dot(recv[g, c], gate_v[h, c * cw : (c + 1) * cw, at])
                up += dot(recv[g, c], up_v[h, c * cw : (c + 1) * cw, at])
            hidden[g, h, :, at] = activate(gate, up)

    def came(g, k, c):
        return r_near.at[min(k, 2)] if g < 2 else r_recv.at[k - 2, c]

    def contract(g, k, t, chunks=(0, CHUNKS)):
        base = own_base + t * (mate_base - own_base)

        @pl.loop(chunks[0] // PAIR, chunks[1] // PAIR)
        def _(p):
            total = jnp.zeros((rows, PAIR * cw), jnp.float32)
            for h in range(tps):
                at = pl.ds(pl.multiple_of(p * PAIR * cw, PAIR * cw), PAIR * cw)
                part = dot(hidden[g, h], down_v[h, :, at])
                total += part.astype(jnp.bfloat16).astype(jnp.float32)
            total = total.astype(jnp.bfloat16)
            for q in range(PAIR):
                recv[g, PAIR * p + q] = total[:, q * cw : (q + 1) * cw]

            @pl.when(t == 0)
            def _():
                for q in range(PAIR):
                    ret[k, PAIR * p + q, 0:cap, :] = total[0:cap, q * cw : (q + 1) * cw]

            for q in range(PAIR):
                c = PAIR * p + q

                @pl.loop(1 - t, pz)
                def _(j):
                    remote(
                        recv.at[g, c, block_of(j)], ret.at[k, c, block_of(j)],
                        r_send.at[g], came(g, k, c), {"ep": ring(base, pz - j)},
                    ).start()

    def mix(k, c):
        return dot(mixers[k, 0], ret[k, c]) + dot(mixers[k, 1], ret[k, c])

    def await_far(g, t, c):
        k = 2 * g - 2 + t
        part = ret.at[k, c] if t else ret.at[k, c, pl.ds(cap, rows - cap)]
        await_bytes(part, came(g, k, c))

    for copy in small_copies:
        copy.wait()
    x_copy.wait()
    squares = jnp.zeros((tokens, 1), jnp.float32)
    for c in every:
        xs = out_ref[:, c * cw : (c + 1) * cw].astype(jnp.float32)
        squares = squares + jnp.sum(xs * xs, axis=-1, keepdims=True)
    scale = lax.rsqrt(squares / width + EPSILON)
    partner = far * inner + mate * outer

    def rows_copy(step, c):
        if step == 0:
            return remote(
                held.at[mine, c], held.at[1 + inner, c], n_send.at[0], n_recv.at[inner, c],
                {"ep": partner},
            )
        return remote(
            held.at[1, c], held.at[3, c], n_send.at[1], n_recv.at[2, c], {"ep": far}
        )

    def meta_copy(step):
        if step == 0:
            return remote(
                meta.at[mine], meta.at[1 + inner], m_send.at[0], m_recv.at[1 + inner],
                {"ep": partner},
            )
        return remote(meta.at[1], meta.at[3], m_send.at[1], m_recv.at[3], {"ep": far})

    def part_copy(kind, c):
        if kind == 2:
            return remote(
                fp_recv.at[1, c], fp_recv.at[1, c], q_send.at[2], q_recv.at[1, c], {"ep": mate}
            )
        return remote(
            fp_send.at[kind, c], fp_recv.at[kind, c], q_send.at[kind], q_recv.at[kind, c],
            {"ep": far},
        )

    def await_rows(g, c):
        await_bytes(held.at[g, c], n_recv.at[g - 1, c])

    def await_meta(g):
        await_bytes(meta.at[g], m_recv.at[g])

    def await_part(kind, c):
        await_bytes(fp_recv.at[kind, c], q_recv.at[kind, c])

    def relay(c):
        await_rows(1, c)
        rows_copy(1, c).start()
        pick(1, 0, c)

    def accept(g, c):
        await_rows(g, c)
        pick(g, 1, c)
        pick(g, 0, c)

    def forward_copy(g, c):
        k = 2 * g - 1
        return remote(
            ret.at[k, c], ret.at[k, c], f_send.at[g - 2], came(g, k, c), {"ep": mate}
        )

    def forward(g, chunks):
        @pl.loop(*chunks)
        def _(c):
            k = 2 * g - 1
            await_bytes(ret.at[k, c, pl.ds(cap, rows - cap)], came(g, k, c))
            forward_copy(g, c).start()

    def share(g, c):
        await_far(g, 0, c)
        await_far(g, 1, c)
        fp_send[g - 2, c] = (mix(2 * g - 2, c) + mix(2 * g - 1, c)).astype(jnp.bfloat16)
        part_copy(g - 2, c).start()

    def await_peers(w):
        for copy in peer_copies[w]:
            copy.wait()

    def normalise(chunks):
        for c in chunks:
            xs = out_ref[:, c * cw : (c + 1) * cw].astype(jnp.float32)
            held[mine, c] = (xs * scale * pre_ref[:, c * cw : (c + 1) * cw]).astype(jnp.bfloat16)

    normalise(range(EARLY))
    meta[mine, 0:2, :] = ids_ref[...].astype(jnp.float32)
    meta[mine, 2:4, :] = route_ref[...]
    meta[mine, 4:8, :] = jnp.zeros((4, tokens), jnp.float32)
    pl.semaphore_wait(barrier, 2 * pz - 1 + tps - 1 + inner)
    meta_copy(0).start()
    for c in range(EARLY):
        rows_copy(0, c).start()
    normalise(range(EARLY, CHUNKS))

    @on_outer
    def _():
        for c in range(EARLY, CHUNKS):
            rows_copy(0, c).start()

    for copies in [local_copies] + peer_copies:
        for copy in copies:
            copy.start()

    place(mine, (0, 1))

    @pl.loop(0, CHUNKS)
    def _(c):
        pick(mine, 0, c)
        on_inner(lambda: pick(0, 1, c))

    @on_inner
    def _():
        await_meta(1)
        meta_copy(1).start()
        place(1, (0,))

        @pl.loop(0, 3)
        def _(c):
            relay(c)

        await_meta(3)
        place(3, (0, 1))
        accept(3, 0)
        prepare(6, 4)
        relay(3)
        prepare(7, 5)
        accept(3, 1)
        received_in_plane(0)
        local_copies[0].wait()
        local_copies[1].wait()
        await_meta(2)
        place(2, (0, 1))
        some = tps * (fh // TILE) // (CHUNKS - 4)

        @pl.loop(4, CHUNKS)
        def _(c):
            relay(c)

            @pl.when(c == CHUNKS - 1)
            def _():
                @pl.loop(EARLY, CHUNKS)
                def _(d):
                    rows_copy(0, d).start()

            accept(3, c - 2)

            @pl.when(c == CHUNKS - 2)
            def _():
                await_peers(0)
                await_peers(1)

            tile = (c - 4) * some
            expand(0, tile // (fh // TILE), lax.rem(tile, fh // TILE), some)

    def accept_all(g, chunks):
        @pl.loop(*chunks)
        def _(c):
            accept(g, c)

    def share_all(g, chunks):
        @pl.loop(*chunks)
        def _(c):
            share(g, c)

    def pass_on(c):
        await_part(1, c)

        @pl.when(c >= STRAIGHT)
        def _():
            value = fp_recv[1, c].astype(jnp.float32) + mix(6, c)
            fp_recv[1, c] = value.astype(jnp.bfloat16)

        part_copy(2, c).start()

    def await_down():
        local_copies[2].wait()
        await_peers(2)

    @on_inner
    def _():
        accept(3, CHUNKS - 2)
        received_in_plane(1)
        expand(1, 0, 0, fh // TILE // 2)
        accept(3, CHUNKS - 1)
        accept_all(2, (0, EARLY))

    @on_outer
    def _():
        received_crossed(0)
        local_copies[0].wait()
        local_copies[1].wait()
        expand(0, 0)
        await_peers(0)
        await_peers(1)
        for i in range(1, tps):
            expand(0, i)
        await_down()
        contract(0, 1, 1, (0, LATER))

    received_part(0)
    begin(0)
    on_inner(lambda: accept(2, 2))
    begin(1)
    on_inner(lambda: accept(2, 3))
    on_inner(await_down)
    received_part(1)
    for i in range(tps):
        complete(i)
    contract(3, 4 + outer, outer, (0, DIRECT))

    @on_outer
    def _():
        contract(3, 5, 0, (DIRECT, CHUNKS))
        received_in_plane(1)
        expand(1, 0)
        forward(3, (DIRECT, LATER))
        contract(0, 1, 1, (LATER, CHUNKS))
        expand(1, 1)

    @on_inner
    def _():
        accept_all(2, (4, 6))
        expand(1, 0, fh // TILE // 2, fh // TILE // 2)
        accept(2, 6)
        share(3, 0)
        expand(1, 1, 0, fh // TILE // 2)
        accept(2, 7)
        expand(1, 1, fh // TILE // 2, fh // TILE // 2)
        share(3, 1)
        contract(1, 1, 1, (0, 4))
        share(3, 2)
        contract(3, 4, 0, (DIRECT, CHUNKS))
        share(3, 3)
        contract(1, 1, 1, (4, STRAIGHT))
        contract(1, 6, 0, (STRAIGHT, CHUNKS))
        prepare(2, 6)
        prepare(4, 2)
        prepare(5, 3)

    received(2)
    expand(2, 0)
    on_inner(lambda: share_all(3, (4, 6)))
    on_outer(lambda: forward(3, (LATER, CHUNKS)))
    expand(2, 1)
    on_inner(lambda: share_all(3, (6, CHUNKS)))
    contract(2, 2 + outer, outer, (0, PAIR))
    contract(2, 2 + outer, 0, (PAIR, CHUNKS))

    @on_outer
    def _():
        forward(2, (PAIR, CHUNKS))
        contract(1, 0, 0)


    @on_inner
    def _():
        @pl.loop(0, 4)
        def _(c):
            pass_on(c)

        share_all(2, (0, 2))
        contract(0, 0, 0)
        some = pl.ds(STRAIGHT, CHUNKS - STRAIGHT)
        await_bytes(ret.at[6, some, pl.ds(cap, rows - cap)], r_near.at[2])

        @pl.loop(2, CHUNKS)
        def _(c):
            share(2, c)
            pl.when(c < CHUNKS - 2)(lambda: pass_on(c + 2))

    def mixed(c):
        per = fh // cw
        at = pl.ds(pl.multiple_of(lax.rem(c, per) * cw, cw), cw)
        return acc.at[c // per, pl.ds(0, tokens), at]

    prepare(2 * mine, 0)
    prepare(2 * mine + 1, 1)
    await_bytes(ret.at[0, :, pl.ds(cap, rows - cap)], r_near.at[0])
    on_inner(lambda: await_bytes(ret.at[1], r_near.at[1]))
    on_outer(lambda: await_bytes(ret.at[1, pl.ds(0, STRAIGHT)], r_near.at[1]))

    @pl.loop(0, STRAIGHT)
    def _(c):
        mixed(c)[...] = mix(0, c) + mix(1, c)

    @pl.loop(STRAIGHT, CHUNKS)
    def _(c):
        mixed(c)[...] = mix(0, c)

        @on_inner
        def _():
            mixed(c)[...] = mixed(c)[...] + mix(1, c)

    meta_copy(0).wait_send()
    on_inner(meta_copy(1).wait_send)
    others = pl.ds(cap, rows - cap)

    def picked(g):
        await_bytes(send.at[sent(g, 0), :, others], d_send.at[sent(g, 0)])

    def in_plane(g):
        await_bytes(recv.at[g, :, others], r_send.at[g])

    picked(mine)
    in_plane(mine)

    @on_inner
    def _():
        await_bytes(held.at[0], n_send.at[0])
        await_bytes(held.at[1], n_send.at[1])
        for g in (1, 2, 3):
            picked(g)
        for g in (2, 3):
            in_plane(g)
        some = pl.ds(STRAIGHT, CHUNKS - STRAIGHT)
        await_bytes(recv.at[1, pl.ds(0, STRAIGHT)], r_send.at[1])
        await_bytes(recv.at[1, some, others], r_send.at[1])
        for g in (0, 2, 3):
            await_bytes(send.at[sent(g, 1)], d_send.at[sent(g, 1)])
        for kind in range(2):
            await_bytes(fp_send.at[kind], q_send.at[kind])

    @on_outer
    def _():
        await_bytes(held.at[1], n_send.at[0])
        await_bytes(recv.at[0], r_send.at[0])
        for g, direct in ((2, PAIR), (3, DIRECT)):
            some = pl.ds(direct, CHUNKS - direct)
            await_bytes(recv.at[g, pl.ds(0, direct)], r_send.at[g])
            await_bytes(recv.at[g, some, others], r_send.at[g])
            await_bytes(ret.at[2 * g - 1, some], f_send.at[g - 2])

    squares = jnp.zeros((tokens, 1), jnp.float32)
    for c in every:
        await_part(mine, c)
        total = mixed(c)[...] + fp_recv[mine, c].astype(jnp.float32)
        mixed(c)[...] = total
        squares = squares + jnp.sum(total * total, axis=-1, keepdims=True)
    scale = lax.rsqrt(squares / width + EPSILON)
    for c in every:
        at = slice(c * cw, (c + 1) * cw)
        out_ref[:, at] = (mixed(c)[...] * scale * post_ref[:, at]).astype(jnp.bfloat16)

    on_inner(lambda: await_bytes(fp_recv.at[1], q_send.at[2]))


def local(inputs, pre_gain, expert_ids, route_weights, gate_proj, up_proj, down_proj, post_gain):
    tokens, width = inputs.shape
    choices = expert_ids.shape[1]
    n = lax.axis_size("ep")
    tps = lax.axis_size("tp")
    cap = 3 * tokens * choices // (2 * n * gate_proj.shape[0])
    cap = -(-cap // 16) * 16
    rows = n // PLANES * cap
    cw = width // CHUNKS
    fh = gate_proj.shape[2]
    bf16, f32 = jnp.bfloat16, jnp.float32
    vmem = pl.BlockSpec(memory_space=pltpu.VMEM)
    hbm = pl.BlockSpec(memory_space=pltpu.HBM)
    dma = pltpu.SemaphoreType.DMA
    return pl.pallas_call(
        functools.partial(kernel, n, tps, cap),
        out_shape=pltpu.VMEM((tokens, width), bf16),
        in_specs=[hbm] * 8,
        out_specs=vmem,
        scratch_shapes=[
            pltpu.VMEM((1, width), f32),
            pltpu.VMEM((choices, tokens), jnp.int32),
            pltpu.VMEM((choices, tokens), f32),
            pltpu.VMEM((1, width), f32),
            pltpu.VMEM((tps, width, fh), bf16),
            pltpu.VMEM((tps, width, fh), bf16),
            pltpu.VMEM((tps, fh, width), bf16),
            pltpu.VMEM((4, CHUNKS, tokens, cw), bf16),
            pltpu.VMEM((4, 8, tokens), f32),
            pltpu.VMEM((7, CHUNKS, rows, cw), bf16),
            pltpu.VMEM((4, CHUNKS, rows, cw), bf16),
            pltpu.VMEM((7, CHUNKS, rows, cw), bf16),
            pltpu.VMEM((2, CHUNKS, tokens, cw), bf16),
            pltpu.VMEM((2, CHUNKS, tokens, cw), bf16),
            pltpu.VMEM((2 * tps, max(rows, tokens), fh), f32),
            pltpu.VMEM((4, tps, rows, fh), bf16),
            pltpu.VMEM((8, 8, tokens), f32),
            pltpu.VMEM((7, 2, tokens, rows), bf16),
            dma, dma((4,)), dma((3,)), dma((3, tps - 1)), dma((3, tps - 1)),
            dma((2,)), dma((3, CHUNKS)), dma((2,)), dma((4,)),
            dma((7,)), dma((5,)), dma((4,)), dma((3,)), dma((4, CHUNKS)),
            dma((2,)), dma((3,)), dma((2, CHUNKS)),
        ],
        compiler_params=pltpu.CompilerParams(
            collective_id=0, has_side_effects=True, vmem_limit_bytes=67043328 - 2**20
        ),
    )(
        inputs, pre_gain[None, :], expert_ids.T, route_weights.T,
        gate_proj, up_proj, down_proj, post_gain[None, :],
    )


def solution(mesh):
    in_specs = (
        P(("ep", "tp"), None),
        P(),
        P(("ep", "tp"), None),
        P(("ep", "tp"), None),
        P("ep", None, "tp"),
        P("ep", None, "tp"),
        P("ep", "tp", None),
        P(),
    )
    out_specs = P(("ep", "tp"), None)
    return jax.shard_map(local, mesh=mesh, in_specs=in_specs, out_specs=out_specs, check_vma=False)
```

```python
import functools

import jax
import jax.numpy as jnp
from jax import lax
from jax.experimental import pallas as pl
from jax.experimental.pallas import tpu as pltpu
from jax.sharding import PartitionSpec as P

EPSILON = 1e-06
LIMIT = 7.0
ALPHA = 1.702
CHUNKS = 8
DIRECT = 4
EARLY = 2
SPLIT = 6
STRAIGHT = 6
LATER = 6
BLOCKS = 4
PAIR = 2
TILE = 256
PLANES = 4
MESH = pl.DeviceIdType.MESH


def activate(gate, up):
    gate = jnp.minimum(gate, LIMIT)
    up = jnp.clip(up, -LIMIT, LIMIT)
    return ((up + 1.0) * gate * jax.nn.sigmoid(ALPHA * gate)).astype(jnp.bfloat16)


def dot(a, b):
    return jnp.dot(a, b, preferred_element_type=jnp.float32)


def kernel(
    n, tps, cap,
    x_hbm, pre_hbm, ids_hbm, route_hbm, gate_ref, up_ref, down_ref, post_hbm, out_ref,
    pre_ref, ids_ref, route_ref, post_ref, gate_v, up_v, down_v, held, meta, send, recv, ret,
    fp_send, fp_recv, acc, hidden, places, mixers,
    x_sem, s_sem, w_local, w_send, w_recv, n_send, n_recv, m_send, m_recv,
    d_send, d_recv, r_send, r_near, r_recv, f_send, q_send, q_recv,
):
    tokens, width = out_ref.shape
    pz = n // PLANES
    cw = width // CHUNKS
    rows = pz * cap
    fh = gate_v.shape[2]
    every = range(CHUNKS)
    me = lax.axis_index("ep")
    core = lax.axis_index("tp")
    plane = me // pz
    column = lax.rem(me, pz)
    inner = plane * (3 - plane) // 2
    outer = 1 - inner
    mine = outer
    mate_base = (plane + 1 - 2 * lax.rem(plane, 2)) * pz
    own_base = plane * pz
    mate = mate_base + column
    far = (3 - plane) * pz + column

    def on_inner(f):
        pl.when(inner == 1)(f)

    def on_outer(f):
        pl.when(inner == 0)(f)

    def ring(base, j):
        return base + lax.rem(column + j, pz)

    def greet(device):
        pl.semaphore_signal(barrier, inc=1, device_id=device, device_id_type=MESH)

    x_copy = pltpu.make_async_copy(x_hbm, out_ref, x_sem)
    x_copy.start()
    small_copies = [
        pltpu.make_async_copy(src, dst, s_sem.at[i])
        for i, (src, dst) in enumerate(
            ((pre_hbm, pre_ref), (ids_hbm, ids_ref), (route_hbm, route_ref), (post_hbm, post_ref))
        )
    ]
    for copy in small_copies:
        copy.start()
    weights = ((gate_ref, gate_v), (up_ref, up_v), (down_ref, down_v))
    local_copies = [
        pltpu.make_async_copy(src.at[0], dst.at[core], w_local.at[w])
        for w, (src, dst) in enumerate(weights)
    ]
    barrier = pltpu.get_barrier_semaphore()

    @pl.loop(1, pz)
    def _(j):
        greet({"ep": ring(own_base, j)})

    @pl.loop(0, pz)
    def _(j):
        greet({"ep": ring(mate_base, j)})

    for i in range(1, tps):
        greet({"tp": lax.rem(core + i, tps)})

    @on_inner
    def _():
        greet({"ep": far})

    def remote(src, dst, ss, rs, where):
        return pltpu.make_async_remote_copy(
            src_ref=src, dst_ref=dst, send_sem=ss, recv_sem=rs,
            device_id=where, device_id_type=MESH,
        )

    def await_bytes(ref, sem):
        pltpu.make_async_copy(ref, ref, sem).wait()

    peer_copies = [
        [
            remote(
                src.at[0], dst.at[core], w_send.at[w, i - 1], w_recv.at[w, i - 1],
                {"tp": lax.rem(core + i, tps)},
            )
            for i in range(1, tps)
        ]
        for w, (src, dst) in enumerate(weights)
    ]
    def place(g, ts):
        values = meta[g]
        experts_col = lax.broadcasted_iota(jnp.int32, (n, 1), 0).astype(jnp.float32)
        earlier = (
            lax.broadcasted_iota(jnp.int32, (tokens, tokens), 0)
            < lax.broadcasted_iota(jnp.int32, (tokens, tokens), 1)
        ).astype(jnp.bfloat16)
        first, second = values[0:1, :], values[1:2, :]
        hot0 = (first == experts_col).astype(jnp.float32)
        hot1 = (second == experts_col).astype(jnp.float32)
        before = dot((hot0 + hot1).astype(jnp.bfloat16), earlier)
        for t in ts:
            start = (mate_base if t else own_base).astype(jnp.float32)
            places[2 * g + t] = values
            for i, (ids, hot) in enumerate(((first, hot0), (second, hot1))):
                slot = jnp.sum(before * hot, axis=0, keepdims=True)
                inside = (ids >= start) & (ids < start + pz)
                relative = ids - (start + column.astype(jnp.float32))
                relative = jnp.where(relative < 0, relative + pz, relative)
                places[2 * g + t, i : i + 1, :] = jnp.where(inside, relative * cap + slot, -1.0)

    def picker(k):
        at = lax.broadcasted_iota(jnp.int32, (rows, 1), 0).astype(jnp.float32)
        return (
            (places[k, 0:1, :] == at).astype(jnp.float32)
            + (places[k, 1:2, :] == at).astype(jnp.float32)
        ).astype(jnp.bfloat16)

    def prepare(k, r):
        columns = places[k].T
        at = lax.broadcasted_iota(jnp.int32, (1, rows), 1).astype(jnp.float32)
        w = jnp.where(columns[:, 0:1] == at, columns[:, 2:3], 0.0) + jnp.where(
            columns[:, 1:2] == at, columns[:, 3:4], 0.0
        )
        high = w.astype(jnp.bfloat16)
        mixers[r, 0] = high
        mixers[r, 1] = (w - high.astype(jnp.float32)).astype(jnp.bfloat16)

    def block_of(j):
        return pl.ds(pl.multiple_of(j * cap, cap), cap)

    def sent(g, t):
        return 2 * g + t - (1 if isinstance(g, int) and g > 1 else 0)

    def pick(g, t, c):
        k = sent(g, t)
        picked = dot(picker(2 * g + t), held[g, c]).astype(jnp.bfloat16)
        if t == 0:
            recv[g, c, 0:cap, :] = picked[0:cap]
            send[k, c, cap:rows, :] = picked[cap:rows]
        else:
            send[k, c] = picked
        base = mate_base if t else own_base
        late = c // SPLIT if isinstance(g, int) and g == 3 else 0

        @pl.loop(1 - t, pz)
        def _(j):
            remote(
                send.at[k, c, block_of(j)], recv.at[g, c, block_of(j)],
                d_send.at[k], d_recv.at[g + late], {"ep": ring(base, j)},
            ).start()

    def received_in_plane(g):
        await_bytes(recv.at[g, :, pl.ds(cap, rows - cap)], d_recv.at[g])

    def received_crossed(g):
        await_bytes(recv.at[g], d_recv.at[g])

    def received(g):
        on_inner(lambda: received_in_plane(g))
        on_outer(lambda: received_crossed(g))

    def received_part(late):
        part = pl.ds(SPLIT * late, SPLIT + late * (CHUNKS - 2 * SPLIT))
        on_inner(lambda: await_bytes(recv.at[3, part, pl.ds(cap, rows - cap)], d_recv.at[3 + late]))
        on_outer(lambda: await_bytes(recv.at[3, part], d_recv.at[3 + late]))

    def begin(i):
        h = lax.rem(core + i, tps)

        @pl.loop(0, fh // TILE)
        def _(t):
            at = pl.ds(pl.multiple_of(t * TILE, TILE), TILE)
            gate = jnp.zeros((rows, TILE), jnp.float32)
            up = jnp.zeros((rows, TILE), jnp.float32)
            for c in range(SPLIT):
                gate += dot(recv[3, c], gate_v[h, c * cw : (c + 1) * cw, at])
                up += dot(recv[3, c], up_v[h, c * cw : (c + 1) * cw, at])
            acc[2 * i, 0:rows, at] = gate
            acc[2 * i + 1, 0:rows, at] = up

    def complete(i):
        h = lax.rem(core + i, tps)

        @pl.loop(0, fh // TILE)
        def _(t):
            at = pl.ds(pl.multiple_of(t * TILE, TILE), TILE)
            gate = jnp.zeros((rows, TILE), jnp.float32)
            up = jnp.zeros((rows, TILE), jnp.float32)
            for c in range(SPLIT, CHUNKS):
                gate += dot(recv[3, c], gate_v[h, c * cw : (c + 1) * cw, at])
                up += dot(recv[3, c], up_v[h, c * cw : (c + 1) * cw, at])
            gate += acc[2 * i, 0:rows, at]
            up += acc[2 * i + 1, 0:rows, at]
            hidden[3, h, :, at] = activate(gate, up)

    def expand(g, i, first=0, tiles=fh // TILE):
        h = lax.rem(core + i, tps)

        @pl.loop(first, first + tiles)
        def _(t):
            at = pl.ds(pl.multiple_of(t * TILE, TILE), TILE)
            gate = jnp.zeros((rows, TILE), jnp.float32)
            up = jnp.zeros((rows, TILE), jnp.float32)
            for c in every:
                gate += dot(recv[g, c], gate_v[h, c * cw : (c + 1) * cw, at])
                up += dot(recv[g, c], up_v[h, c * cw : (c + 1) * cw, at])
            hidden[g, h, :, at] = activate(gate, up)

    def came(g, k, c):
        return r_near.at[min(k, 2)] if g < 2 else r_recv.at[k - 2, c]

    def contract(g, k, t, chunks=(0, CHUNKS)):
        base = own_base + t * (mate_base - own_base)

        @pl.loop(chunks[0] // PAIR, chunks[1] // PAIR)
        def _(p):
            total = jnp.zeros((rows, PAIR * cw), jnp.float32)
            for h in range(tps):
                at = pl.ds(pl.multiple_of(p * PAIR * cw, PAIR * cw), PAIR * cw)
                part = dot(hidden[g, h], down_v[h, :, at])
                total += part.astype(jnp.bfloat16).astype(jnp.float32)
            total = total.astype(jnp.bfloat16)
            for q in range(PAIR):
                recv[g, PAIR * p + q] = total[:, q * cw : (q + 1) * cw]

            @pl.when(t == 0)
            def _():
                for q in range(PAIR):
                    ret[k, PAIR * p + q, 0:cap, :] = total[0:cap, q * cw : (q + 1) * cw]

            for q in range(PAIR):
                c = PAIR * p + q

                @pl.loop(1 - t, pz)
                def _(j):
                    remote(
                        recv.at[g, c, block_of(j)], ret.at[k, c, block_of(j)],
                        r_send.at[g], came(g, k, c), {"ep": ring(base, pz - j)},
                    ).start()

    def mix(k, c):
        return dot(mixers[k, 0], ret[k, c]) + dot(mixers[k, 1], ret[k, c])

    def await_far(g, t, c):
        k = 2 * g - 2 + t
        part = ret.at[k, c] if t else ret.at[k, c, pl.ds(cap, rows - cap)]
        await_bytes(part, came(g, k, c))

    for copy in small_copies:
        copy.wait()
    x_copy.wait()
    squares = jnp.zeros((tokens, 1), jnp.float32)
    for c in every:
        xs = out_ref[:, c * cw : (c + 1) * cw].astype(jnp.float32)
        squares = squares + jnp.sum(xs * xs, axis=-1, keepdims=True)
    scale = lax.rsqrt(squares / width + EPSILON)
    partner = far * inner + mate * outer

    def rows_copy(step, c):
        if step == 0:
            return remote(
                held.at[mine, c], held.at[1 + inner, c], n_send.at[0], n_recv.at[inner, c],
                {"ep": partner},
            )
        return remote(
            held.at[1, c], held.at[3, c], n_send.at[1], n_recv.at[2, c], {"ep": far}
        )

    def meta_copy(step):
        if step == 0:
            return remote(
                meta.at[mine], meta.at[1 + inner], m_send.at[0], m_recv.at[1 + inner],
                {"ep": partner},
            )
        return remote(meta.at[1], meta.at[3], m_send.at[1], m_recv.at[3], {"ep": far})

    def part_copy(kind, c):
        if kind == 2:
            return remote(
                fp_recv.at[1, c], fp_recv.at[1, c], q_send.at[2], q_recv.at[1, c], {"ep": mate}
            )
        return remote(
            fp_send.at[kind, c], fp_recv.at[kind, c], q_send.at[kind], q_recv.at[kind, c],
            {"ep": far},
        )

    def await_rows(g, c):
        await_bytes(held.at[g, c], n_recv.at[g - 1, c])

    def await_meta(g):
        await_bytes(meta.at[g], m_recv.at[g])

    def await_part(kind, c):
        await_bytes(fp_recv.at[kind, c], q_recv.at[kind, c])

    def relay(c):
        await_rows(1, c)
        rows_copy(1, c).start()
        pick(1, 0, c)

    def accept(g, c):
        await_rows(g, c)
        pick(g, 1, c)
        pick(g, 0, c)

    def forward_copy(g, c):
        k = 2 * g - 1
        return remote(
            ret.at[k, c], ret.at[k, c], f_send.at[g - 2], came(g, k, c), {"ep": mate}
        )

    def forward(g, chunks):
        @pl.loop(*chunks)
        def _(c):
            k = 2 * g - 1
            await_bytes(ret.at[k, c, pl.ds(cap, rows - cap)], came(g, k, c))
            forward_copy(g, c).start()

    def share(g, c):
        await_far(g, 0, c)
        await_far(g, 1, c)
        fp_send[g - 2, c] = (mix(2 * g - 2, c) + mix(2 * g - 1, c)).astype(jnp.bfloat16)
        part_copy(g - 2, c).start()

    def await_peers(w):
        for copy in peer_copies[w]:
            copy.wait()

    def normalise(chunks):
        for c in chunks:
            xs = out_ref[:, c * cw : (c + 1) * cw].astype(jnp.float32)
            held[mine, c] = (xs * scale * pre_ref[:, c * cw : (c + 1) * cw]).astype(jnp.bfloat16)

    normalise(range(EARLY))
    meta[mine, 0:2, :] = ids_ref[...].astype(jnp.float32)
    meta[mine, 2:4, :] = route_ref[...]
    meta[mine, 4:8, :] = jnp.zeros((4, tokens), jnp.float32)
    pl.semaphore_wait(barrier, 2 * pz - 1 + tps - 1 + inner)
    meta_copy(0).start()
    for c in range(EARLY):
        rows_copy(0, c).start()
    normalise(range(EARLY, CHUNKS))

    @on_outer
    def _():
        for c in range(EARLY, CHUNKS):
            rows_copy(0, c).start()

    for copies in [local_copies] + peer_copies:
        for copy in copies:
            copy.start()

    place(mine, (0, 1))

    @pl.loop(0, CHUNKS)
    def _(c):
        on_inner(lambda: pick(0, 1, c))
        pick(mine, 0, c)

    @on_inner
    def _():
        await_meta(1)
        meta_copy(1).start()
        place(1, (0,))

        @pl.loop(0, 3)
        def _(c):
            relay(c)

        await_meta(3)
        place(3, (0, 1))
        accept(3, 0)
        prepare(6, 4)
        relay(3)
        prepare(7, 5)
        accept(3, 1)
        received_in_plane(0)
        local_copies[0].wait()
        local_copies[1].wait()
        await_meta(2)
        place(2, (0, 1))
        some = tps * (fh // TILE) // (CHUNKS - 4)

        @pl.loop(4, CHUNKS)
        def _(c):
            relay(c)

            @pl.when(c == CHUNKS - 1)
            def _():
                @pl.loop(EARLY, CHUNKS)
                def _(d):
                    rows_copy(0, d).start()

            accept(3, c - 2)

            @pl.when(c == CHUNKS - 2)
            def _():
                await_peers(0)
                await_peers(1)

            tile = (c - 4) * some
            expand(0, tile // (fh // TILE), lax.rem(tile, fh // TILE), some)

    def accept_all(g, chunks):
        @pl.loop(*chunks)
        def _(c):
            accept(g, c)

    def share_all(g, chunks):
        @pl.loop(*chunks)
        def _(c):
            share(g, c)

    def pass_on(c):
        await_part(1, c)

        @pl.when(c >= STRAIGHT)
        def _():
            value = fp_recv[1, c].astype(jnp.float32) + mix(6, c)
            fp_recv[1, c] = value.astype(jnp.bfloat16)

        part_copy(2, c).start()

    def await_down():
        local_copies[2].wait()
        await_peers(2)

    @on_inner
    def _():
        accept(3, CHUNKS - 2)
        received_in_plane(1)
        expand(1, 0, 0, fh // TILE // 2)
        accept(3, CHUNKS - 1)
        accept_all(2, (0, EARLY))

    @on_outer
    def _():
        received_crossed(0)
        local_copies[0].wait()
        local_copies[1].wait()
        expand(0, 0)
        await_peers(0)
        await_peers(1)
        for i in range(1, tps):
            expand(0, i)
        await_down()
        contract(0, 1, 1, (0, LATER))

    received_part(0)
    begin(0)
    on_inner(lambda: accept(2, 2))
    begin(1)
    on_inner(lambda: accept(2, 3))
    on_inner(await_down)
    received_part(1)
    for i in range(tps):
        complete(i)
    contract(3, 4 + outer, outer, (0, DIRECT))

    @on_outer
    def _():
        contract(3, 5, 0, (DIRECT, CHUNKS))
        received_in_plane(1)
        expand(1, 0)
        forward(3, (DIRECT, LATER))
        contract(0, 1, 1, (LATER, CHUNKS))
        expand(1, 1)

    @on_inner
    def _():
        accept_all(2, (4, 6))
        expand(1, 0, fh // TILE // 2, fh // TILE // 2)
        accept(2, 6)
        share(3, 0)
        expand(1, 1, 0, fh // TILE // 2)
        accept(2, 7)
        expand(1, 1, fh // TILE // 2, fh // TILE // 2)
        share(3, 1)
        contract(1, 1, 1, (0, 4))
        share(3, 2)
        contract(3, 4, 0, (DIRECT, CHUNKS))
        share(3, 3)
        contract(1, 1, 1, (4, STRAIGHT))
        contract(1, 6, 0, (STRAIGHT, CHUNKS))
        prepare(2, 6)
        prepare(4, 2)
        prepare(5, 3)

    received(2)
    expand(2, 0)
    on_inner(lambda: share_all(3, (4, 6)))
    on_outer(lambda: forward(3, (LATER, CHUNKS)))
    expand(2, 1)
    on_inner(lambda: share_all(3, (6, CHUNKS)))
    contract(2, 2 + outer, outer, (0, PAIR))
    contract(2, 2 + outer, 0, (PAIR, CHUNKS))

    @on_outer
    def _():
        forward(2, (PAIR, CHUNKS))
        contract(1, 0, 0)


    @on_inner
    def _():
        @pl.loop(0, 4)
        def _(c):
            pass_on(c)

        share_all(2, (0, 2))
        contract(0, 0, 0)
        some = pl.ds(STRAIGHT, CHUNKS - STRAIGHT)
        await_bytes(ret.at[6, some, pl.ds(cap, rows - cap)], r_near.at[2])

        @pl.loop(2, CHUNKS)
        def _(c):
            share(2, c)
            pl.when(c < CHUNKS - 2)(lambda: pass_on(c + 2))

    def mixed(c):
        per = fh // cw
        at = pl.ds(pl.multiple_of(lax.rem(c, per) * cw, cw), cw)
        return acc.at[c // per, pl.ds(0, tokens), at]

    prepare(2 * mine, 0)
    prepare(2 * mine + 1, 1)
    await_bytes(ret.at[0, :, pl.ds(cap, rows - cap)], r_near.at[0])
    on_inner(lambda: await_bytes(ret.at[1], r_near.at[1]))
    on_outer(lambda: await_bytes(ret.at[1, pl.ds(0, STRAIGHT)], r_near.at[1]))

    @pl.loop(0, STRAIGHT)
    def _(c):
        mixed(c)[...] = mix(0, c) + mix(1, c)

    @pl.loop(STRAIGHT, CHUNKS)
    def _(c):
        mixed(c)[...] = mix(0, c)

        @on_inner
        def _():
            mixed(c)[...] = mixed(c)[...] + mix(1, c)

    meta_copy(0).wait_send()
    on_inner(meta_copy(1).wait_send)
    others = pl.ds(cap, rows - cap)

    def picked(g):
        await_bytes(send.at[sent(g, 0), :, others], d_send.at[sent(g, 0)])

    def in_plane(g):
        await_bytes(recv.at[g, :, others], r_send.at[g])

    picked(mine)
    in_plane(mine)

    @on_inner
    def _():
        await_bytes(held.at[0], n_send.at[0])
        await_bytes(held.at[1], n_send.at[1])
        for g in (1, 2, 3):
            picked(g)
        for g in (2, 3):
            in_plane(g)
        some = pl.ds(STRAIGHT, CHUNKS - STRAIGHT)
        await_bytes(recv.at[1, pl.ds(0, STRAIGHT)], r_send.at[1])
        await_bytes(recv.at[1, some, others], r_send.at[1])
        for g in (0, 2, 3):
            await_bytes(send.at[sent(g, 1)], d_send.at[sent(g, 1)])
        for kind in range(2):
            await_bytes(fp_send.at[kind], q_send.at[kind])

    @on_outer
    def _():
        await_bytes(held.at[1], n_send.at[0])
        await_bytes(recv.at[0], r_send.at[0])
        for g, direct in ((2, PAIR), (3, DIRECT)):
            some = pl.ds(direct, CHUNKS - direct)
            await_bytes(recv.at[g, pl.ds(0, direct)], r_send.at[g])
            await_bytes(recv.at[g, some, others], r_send.at[g])
            await_bytes(ret.at[2 * g - 1, some], f_send.at[g - 2])

    squares = jnp.zeros((tokens, 1), jnp.float32)
    for c in every:
        await_part(mine, c)
        total = mixed(c)[...] + fp_recv[mine, c].astype(jnp.float32)
        mixed(c)[...] = total
        squares = squares + jnp.sum(total * total, axis=-1, keepdims=True)
    scale = lax.rsqrt(squares / width + EPSILON)
    for c in every:
        at = slice(c * cw, (c + 1) * cw)
        out_ref[:, at] = (mixed(c)[...] * scale * post_ref[:, at]).astype(jnp.bfloat16)

    on_inner(lambda: await_bytes(fp_recv.at[1], q_send.at[2]))


def local(inputs, pre_gain, expert_ids, route_weights, gate_proj, up_proj, down_proj, post_gain):
    tokens, width = inputs.shape
    choices = expert_ids.shape[1]
    n = lax.axis_size("ep")
    tps = lax.axis_size("tp")
    cap = 3 * tokens * choices // (2 * n * gate_proj.shape[0])
    cap = -(-cap // 16) * 16
    rows = n // PLANES * cap
    cw = width // CHUNKS
    fh = gate_proj.shape[2]
    bf16, f32 = jnp.bfloat16, jnp.float32
    vmem = pl.BlockSpec(memory_space=pltpu.VMEM)
    hbm = pl.BlockSpec(memory_space=pltpu.HBM)
    dma = pltpu.SemaphoreType.DMA
    return pl.pallas_call(
        functools.partial(kernel, n, tps, cap),
        out_shape=pltpu.VMEM((tokens, width), bf16),
        in_specs=[hbm] * 8,
        out_specs=vmem,
        scratch_shapes=[
            pltpu.VMEM((1, width), f32),
            pltpu.VMEM((choices, tokens), jnp.int32),
            pltpu.VMEM((choices, tokens), f32),
            pltpu.VMEM((1, width), f32),
            pltpu.VMEM((tps, width, fh), bf16),
            pltpu.VMEM((tps, width, fh), bf16),
            pltpu.VMEM((tps, fh, width), bf16),
            pltpu.VMEM((4, CHUNKS, tokens, cw), bf16),
            pltpu.VMEM((4, 8, tokens), f32),
            pltpu.VMEM((7, CHUNKS, rows, cw), bf16),
            pltpu.VMEM((4, CHUNKS, rows, cw), bf16),
            pltpu.VMEM((7, CHUNKS, rows, cw), bf16),
            pltpu.VMEM((2, CHUNKS, tokens, cw), bf16),
            pltpu.VMEM((2, CHUNKS, tokens, cw), bf16),
            pltpu.VMEM((2 * tps, max(rows, tokens), fh), f32),
            pltpu.VMEM((4, tps, rows, fh), bf16),
            pltpu.VMEM((8, 8, tokens), f32),
            pltpu.VMEM((7, 2, tokens, rows), bf16),
            dma, dma((4,)), dma((3,)), dma((3, tps - 1)), dma((3, tps - 1)),
            dma((2,)), dma((3, CHUNKS)), dma((2,)), dma((4,)),
            dma((7,)), dma((5,)), dma((4,)), dma((3,)), dma((4, CHUNKS)),
            dma((2,)), dma((3,)), dma((2, CHUNKS)),
        ],
        compiler_params=pltpu.CompilerParams(
            collective_id=0, has_side_effects=True, vmem_limit_bytes=67043328 - 2**20
        ),
    )(
        inputs, pre_gain[None, :], expert_ids.T, route_weights.T,
        gate_proj, up_proj, down_proj, post_gain[None, :],
    )


def solution(mesh):
    in_specs = (
        P(("ep", "tp"), None),
        P(),
        P(("ep", "tp"), None),
        P(("ep", "tp"), None),
        P("ep", None, "tp"),
        P("ep", None, "tp"),
        P("ep", "tp", None),
        P(),
    )
    out_specs = P(("ep", "tp"), None)
    return jax.shard_map(local, mesh=mesh, in_specs=in_specs, out_specs=out_specs, check_vma=False)
```
